32 devices in a mesh: sp: 8 (over z, core), tp: 4 (over y, x).
Axes of the slice: x: 2, y: 2, z: 4, core: 2. Of those that a mesh axis runs over, the one named last changes fastest.
Arguments:
- residual: bfloat16 [3072, 2048], P('sp', 'tp'), may hold values from -40 to 40
- norm_gain: bfloat16 [3, 2048], P(None, 'tp'), may hold values from 0.099609375 to 1.8984375
- w_query: bfloat16 [3, 2048, 2048], P(None, 'tp'), may hold values from -2 to 2
- w_key: bfloat16 [3, 2048, 2048], P(None, 'tp'), may hold values from -8 to 8
- w_value: bfloat16 [3, 2048, 2048], P(None, 'tp'), may hold values from -0.125 to 0.125
- w_out: bfloat16 [3, 2048, 2048], P(None, 'tp'), may hold values from -0.25 to 0.25
- offset_bias: float32 [3, 32, 15, 31], P(None, 'tp'), may hold values from -5 to 5
Outputs:
- out_residual: bfloat16 [3072, 2048], P('sp', 'tp')
The draws below stay inside these ranges and needn't reach their ends.
All inputs are finite; a program needn't handle non-finite values.
Results may differ from the reference program's by a relative error of at most 0.014.
Values may be sent and summed in bfloat16 or wider, within the bound.
A program may use at most 128 MiB of HBM per device.

```python
import math
import jax
import jax.numpy as jnp
from jax import lax

D = 2048
HEADS = 32
HEAD_DIM = 64
GRID_W = 64
NA_ROWS = 8
NA_COLS = 16
LAYERS = 3
NA_W = 2048
ROWS = 48
TOKENS = 3072


def draw_residual(key, part):
    key_one, key_two = jax.random.split(jax.random.fold_in(key, 3), 2)
    ramp = jnp.arange(D, dtype=jnp.float32) / max(D - 1, 1)
    col_scale = jnp.exp(math.log(6.0) * ramp) / 2.5 * jnp.exp(jax.random.uniform(key_two, (D,), jnp.float32, -0.7, 0.7))
    values = jnp.clip(jax.random.normal(key_one, (TOKENS, D), jnp.float32), -4.0, 4.0)
    result = values * col_scale
    return result.astype(jnp.bfloat16)


def query_key_pair(key):
    key_query, key_key = jax.random.split(jax.random.fold_in(key, 11), 2)
    std = D ** (-0.5)
    query_w = jnp.clip(jax.random.normal(key_query, (LAYERS, NA_W, D), jnp.float32), -5.0, 5.0) * std
    key_w = jnp.clip(jax.random.normal(key_key, (LAYERS, NA_W, D), jnp.float32), -5.0, 5.0) * std
    return (query_w, key_w)


def draw_w_query(key, part):
    return query_key_pair(key)[0].astype(jnp.bfloat16)


def draw_w_key(key, part):
    return query_key_pair(key)[1].astype(jnp.bfloat16)


def block_scale(rng, extent, shards, smallest, largest):
    gain = 1.0
    for axis_at, parts in shards:
        draws = jax.random.uniform(jax.random.fold_in(jax.random.fold_in(rng, 6), axis_at), (parts,), jnp.float32, smallest / len(shards), largest / len(shards))
        gain = gain * jnp.repeat(jnp.exp(draws), extent[axis_at] // parts).reshape((-1,) + (1,) * (len(extent) - 1 - axis_at))
    return gain


def gaussian(rng, shape, scale, limit, shards=(), kind=jnp.bfloat16):
    drawn = jax.random.normal(rng, shape, jnp.float32) * scale
    if len(shards) > 0:
        drawn = block_scale(rng, shape, shards, -0.22, 0.18) * drawn
    return jnp.clip(drawn, min=-limit, max=limit).astype(kind)


def setup_inputs(seed: int = 0) -> dict:
    seeds = jax.random.split(jax.random.key(seed), 8)
    return {
        "residual": draw_residual(jax.random.fold_in(seeds[7], 71), 0),
        "norm_gain": jnp.clip(1.0 + 0.18 * jax.random.normal(seeds[1], (LAYERS, D), jnp.float32), 0.099609375, 1.8984375).astype(jnp.bfloat16),
        "w_query": draw_w_query(jax.random.fold_in(seeds[7], 71), 0),
        "w_key": draw_w_key(jax.random.fold_in(seeds[7], 71), 0),
        "w_value": gaussian(seeds[4], (LAYERS, NA_W, D), D ** -0.5, 0.125, ((1, 4),)),
        "w_out": gaussian(seeds[5], (LAYERS, D, NA_W), (NA_W // 4) ** -0.5, 0.25, ((1, 4),)),
        "offset_bias": gaussian(seeds[6], (LAYERS, HEADS, 2 * NA_ROWS - 1, 2 * NA_COLS - 1), 1.0, 5.0, ((1, 4),), jnp.float32),
    }


epsilon = 1e-06

def attend(queries, keys, values, lookup):
    rows_all = ROWS
    query_grid = queries.reshape(rows_all, GRID_W, HEADS, HEAD_DIM)
    key_grid = keys.reshape(rows_all, GRID_W, HEADS, HEAD_DIM)
    value_grid = values.reshape(rows_all, GRID_W, HEADS, HEAD_DIM)
    columns = jnp.arange(GRID_W, dtype=jnp.int32)
    col_index = jnp.clip(columns - NA_COLS // 2, 0, GRID_W - NA_COLS)[:, None] + jnp.arange(NA_COLS, dtype=jnp.int32)
    col_offset = col_index - columns[:, None] + (NA_COLS - 1)

    def row_block(row_global):
        first_row = jnp.clip(row_global - NA_ROWS // 2, 0, rows_all - NA_ROWS).astype(jnp.int32)
        query_row = lax.dynamic_index_in_dim(query_grid, row_global, 0, keepdims=False).astype(jnp.float32)
        key_window = lax.dynamic_slice_in_dim(key_grid, first_row, NA_ROWS, 0)[:, col_index].astype(jnp.float32)
        value_window = lax.dynamic_slice_in_dim(value_grid, first_row, NA_ROWS, 0)[:, col_index].astype(jnp.float32)
        row_offset = first_row + jnp.arange(NA_ROWS, dtype=jnp.int32) - row_global + (NA_ROWS - 1)
        bias_terms = lookup[:, row_offset[:, None, None], col_offset[None, :, :]].transpose(0, 2, 1, 3)
        scores = jnp.einsum('whd,rwkhd->hwrk', query_row, key_window) * HEAD_DIM ** (-0.5) + bias_terms
        weights = jax.nn.softmax(scores.reshape(HEADS, GRID_W, NA_ROWS * NA_COLS), axis=-1).astype(jnp.bfloat16)
        weights = lax.optimization_barrier(weights).astype(jnp.float32).reshape(HEADS, GRID_W, NA_ROWS, NA_COLS)
        attended = jnp.einsum('hwrk,rwkhd->whd', weights, value_window)
        return attended.astype(jnp.bfloat16).reshape(GRID_W, NA_W)
    return lax.map(row_block, jnp.arange(rows_all, dtype=jnp.int32)).reshape(rows_all * GRID_W, NA_W)

def reference(residual, norm_gain, w_query, w_key, w_value, w_out, offset_bias):
    stream = residual
    for layer_index in range(LAYERS):
        res_float = stream.astype(jnp.float32)
        mean_square = lax.optimization_barrier(jnp.mean(res_float * res_float, axis=1, keepdims=True))
        normed = (res_float * lax.rsqrt(mean_square + epsilon) * norm_gain[layer_index].astype(jnp.float32)).astype(jnp.bfloat16)
        queries = jnp.dot(normed, w_query[layer_index].T, preferred_element_type=jnp.float32).astype(jnp.bfloat16)
        keys = jnp.dot(normed, w_key[layer_index].T, preferred_element_type=jnp.float32).astype(jnp.bfloat16)
        values = jnp.dot(normed, w_value[layer_index].T, preferred_element_type=jnp.float32).astype(jnp.bfloat16)
        queries, keys, values = lax.optimization_barrier((queries, keys, values))
        attended = attend(queries, keys, values, offset_bias[layer_index])
        mixed = jnp.dot(attended, w_out[layer_index].T, preferred_element_type=jnp.float32)
        stream = (res_float + mixed).astype(jnp.bfloat16)
    return stream
```

```python
import jax
import jax.numpy as jnp
from jax import lax
from jax.experimental import pallas as pl
from jax.experimental.pallas import tpu as pltpu
from jax.sharding import PartitionSpec as P

HEAD_DIM = 64
GRID_W = 64
NA_ROWS = 8
NA_COLS = 16
LAYERS = 3


epsilon = 1e-06


def padded_2(array, sides, width):
    for axis, dim in sides:
        size, length = (lax.axis_size(axis), array.shape[dim])
        up = [(i, (i + 1) % size) for i in range(size - 1)]
        down = [(j, i) for i, j in up]
        last = lax.slice_in_dim(array, length - width, length, axis=dim)
        first = lax.slice_in_dim(array, 0, width, axis=dim)
        before = lax.ppermute(last, axis, up)
        after = lax.ppermute(first, axis, down)
        array = jnp.concatenate([before, array, after], axis=dim)
    return array


def shortened(array):
    return jax.tree.map(lambda a: a.astype(jnp.bfloat16) if a.dtype == jnp.float32 else a, array)


def contract(left, right):
    return lax.dot_general(
        left, right, (((1,), (1,)), ((), ())), preferred_element_type=jnp.float32
    )


def generic_device(residual, norm_gain, w_query, w_key, w_value, w_out, offset_bias):
    token_count = residual.shape[0]
    local_feats = residual.shape[1]
    local_heads = offset_bias.shape[1]
    head_cols = local_heads * HEAD_DIM
    rows_dev = token_count // GRID_W
    rows_all = rows_dev * lax.axis_size("sp")
    row_base = lax.axis_index("sp") * rows_dev
    reach = NA_ROWS // 2
    slab_width = min(2 * NA_COLS, GRID_W)
    tile_starts = list(range(0, GRID_W, NA_COLS))
    slab_starts = [min(max(start - NA_COLS // 2, 0), GRID_W - slab_width) for start in tile_starts]
    tile_info = []
    for start, slab in zip(tile_starts, slab_starts):
        query_cols = start + jnp.arange(NA_COLS, dtype=jnp.int32)
        key_cols = slab + jnp.arange(slab_width, dtype=jnp.int32)
        first_col = jnp.clip(query_cols - NA_COLS // 2, 0, GRID_W - NA_COLS)
        inside = (key_cols[None, :] >= first_col[:, None]) & (
            key_cols[None, :] < first_col[:, None] + NA_COLS
        )
        offsets = key_cols[None, :] - query_cols[:, None] + (NA_COLS - 1)
        onehot = (offsets[:, :, None] == jnp.arange(2 * NA_COLS - 1, dtype=jnp.int32)).astype(
            jnp.float32
        )
        tile_info.append((start, slab, inside, onehot))
    stream = residual
    for layer_index in range(LAYERS):
        res_float = stream.astype(jnp.float32)
        gathered, gain_all = (
            lax.all_gather(stream, "tp", axis=1, tiled=True),
            lax.all_gather(norm_gain[layer_index][None, :], "tp", axis=1, tiled=True),
        )
        full_float = gathered.astype(jnp.float32)
        inverse = lax.rsqrt(jnp.mean(full_float * full_float, axis=1, keepdims=True) + epsilon)
        normed_all = (full_float * inverse * gain_all.astype(jnp.float32)).astype(jnp.bfloat16)
        queries = contract(normed_all, w_query[layer_index])
        keys = contract(normed_all, w_key[layer_index])
        values = contract(normed_all, w_value[layer_index])
        queries = queries.astype(jnp.bfloat16)
        key_value = jnp.concatenate(
            [keys.astype(jnp.bfloat16), values.astype(jnp.bfloat16)], axis=1
        )
        padded = padded_2(key_value, (("sp", 0),), reach * GRID_W)
        key_grid = padded.reshape(rows_dev + 2 * reach, GRID_W, 2, local_heads, HEAD_DIM)
        query_grid = queries.reshape(rows_dev, GRID_W, local_heads, HEAD_DIM)
        lookup = offset_bias[layer_index]

        def one_row(row_index, query_row):
            row_global = row_base + row_index
            first_row = jnp.clip(row_global - reach, 0, rows_all - NA_ROWS)
            local_first = first_row - row_base + reach
            window = lax.dynamic_slice_in_dim(key_grid, local_first, NA_ROWS, 0)
            row_offset = (
                first_row + jnp.arange(NA_ROWS, dtype=jnp.int32) - row_global + (NA_ROWS - 1)
            )
            row_onehot = (
                row_offset[:, None] == jnp.arange(2 * NA_ROWS - 1, dtype=jnp.int32)
            ).astype(jnp.float32)
            row_bias = jnp.einsum(
                "hab,ra->hrb", lookup, row_onehot, precision=lax.Precision.HIGHEST
            )
            pieces = []
            for start, slab, inside, onehot in tile_info:
                query_tile = query_row[start : start + NA_COLS]
                slab_keys = window[:, slab : slab + slab_width, 0]
                slab_values = window[:, slab : slab + slab_width, 1]
                bias_terms = jnp.einsum(
                    "hrb,wsb->hwrs", row_bias, onehot, precision=lax.Precision.HIGHEST
                )
                scores = jnp.einsum(
                    "whd,rshd->hwrs", query_tile, slab_keys, preferred_element_type=jnp.float32
                )
                scores = scores * HEAD_DIM ** (-0.5) + bias_terms
                scores = jnp.where(inside[None, :, None, :], scores, -jnp.inf)
                weights = jax.nn.softmax(
                    scores.reshape(local_heads, NA_COLS, NA_ROWS * slab_width), axis=-1
                ).astype(jnp.bfloat16)
                weights = weights.reshape(local_heads, NA_COLS, NA_ROWS, slab_width)
                attended = jnp.einsum(
                    "hwrs,rshd->whd", weights, slab_values, preferred_element_type=jnp.float32
                )
                pieces.append(attended.astype(jnp.bfloat16).reshape(NA_COLS, head_cols))
            return jnp.concatenate(pieces, axis=0)

        attended = jax.vmap(one_row)(jnp.arange(rows_dev, dtype=jnp.int32), query_grid).reshape(
            token_count, head_cols
        )
        portion = jax.tree.map(
            lambda part: lax.all_gather(part, "tp", axis=1, tiled=True), shortened(attended)
        )
        out_rows = lax.slice_in_dim(w_out[layer_index], 0, portion.shape[1], axis=1)
        mixed = jnp.zeros((token_count, local_feats), jnp.float32) + contract(portion, out_rows)
        stream = (res_float + mixed).astype(jnp.bfloat16)
    return stream


def bias_lanes(offset_bias):
    layers, heads, row_offs, col_offs = offset_bias.shape
    flipped = jnp.flip(offset_bias, axis=3)
    padded = jnp.pad(flipped, ((0, 0), (0, 0), (0, 1), (0, GRID_W - col_offs)))
    paired = padded.reshape(layers, heads // 2, 2, row_offs + 1, GRID_W)
    return paired.transpose(0, 1, 3, 2, 4).reshape(layers, heads // 2, row_offs + 1, 2 * GRID_W)


def window_mask():
    shape = (GRID_W, 2 * GRID_W)
    key_col = lax.broadcasted_iota(jnp.int32, shape, 0)
    query_col = lax.broadcasted_iota(jnp.int32, shape, 1) % GRID_W
    first = jnp.clip(query_col - NA_COLS // 2, 0, GRID_W - NA_COLS)
    return (key_col >= first) & (key_col < first + NA_COLS)


def build_table(lanes_of, table):
    inside = window_mask()
    for off in range(2 * NA_ROWS - 1):
        row = jnp.broadcast_to(lanes_of(off), (GRID_W, 2 * GRID_W))
        rolled = pltpu.roll(row, 2 * GRID_W - (NA_COLS - 1), axis=1, stride=1, stride_axis=0)
        table[off * GRID_W : (off + 1) * GRID_W, :] = jnp.where(inside, rolled, -1e30)


def attend_row(query, window_keys, window_values, bias):
    low = lax.broadcasted_iota(jnp.int32, query.shape, 1) < HEAD_DIM
    zero = jnp.zeros_like(query)
    block = jnp.concatenate([jnp.where(low, query, zero), jnp.where(low, zero, query)], axis=0)
    scores = contract(window_keys, block) + bias
    top = jnp.max(scores, axis=0, keepdims=True)
    weights = jnp.exp(scores - top)
    inverse = 1.0 / jnp.sum(weights, axis=0, keepdims=True)
    weights = (weights * inverse).astype(jnp.bfloat16)
    mixed = lax.dot_general(
        weights, window_values, (((0,), (0,)), ((), ())), preferred_element_type=jnp.float32
    )
    return jnp.where(low, mixed[:GRID_W], mixed[GRID_W:]).astype(jnp.bfloat16)


def row_window(row, rows_dev, rows_all):
    reach = NA_ROWS // 2
    row_base = lax.axis_index("sp") * rows_dev
    first = jnp.clip(row_base + row - reach, 0, rows_all - NA_ROWS)
    return first - row_base + reach, first - row_base - row + NA_ROWS - 1


def attention_kernel(rows_dev, rows_all, q_ref, kv_ref, lanes_ref, out_ref, table):
    width = q_ref.shape[1]
    for pair in range(width // 128):
        build_table(lambda off: lanes_ref[pair, off : off + 1, :], table)
        cols = slice(pair * 128, (pair + 1) * 128)
        vcols = slice(width + pair * 128, width + (pair + 1) * 128)

        def one_row(row, carry):
            start, off = row_window(row, rows_dev, rows_all)
            keys = pl.ds(pl.multiple_of(start * GRID_W, GRID_W), NA_ROWS * GRID_W)
            here = pl.ds(pl.multiple_of(row * GRID_W, GRID_W), GRID_W)
            bias = table[pl.ds(pl.multiple_of(off * GRID_W, GRID_W), NA_ROWS * GRID_W), :]
            out_ref[here, cols] = attend_row(
                q_ref[here, cols], kv_ref[keys, cols], kv_ref[keys, vcols], bias
            )
            return carry

        lax.fori_loop(0, rows_dev, one_row, 0)


def attention(queries, padded, lanes, rows_dev, rows_all):
    vmem = pl.BlockSpec(memory_space=pltpu.VMEM)
    return pl.pallas_call(
        lambda *refs: attention_kernel(rows_dev, rows_all, *refs),
        out_shape=jax.ShapeDtypeStruct(queries.shape, jnp.bfloat16),
        in_specs=[vmem] * 3,
        out_specs=vmem,
        scratch_shapes=[pltpu.VMEM(((2 * NA_ROWS - 1) * GRID_W, 2 * GRID_W), jnp.float32)],
        name="attention",
    )(queries, padded, lanes)


def paired_device(residual, norm_gain, w_query, w_key, w_value, w_out, offset_bias):
    token_count = residual.shape[0]
    rows_dev = token_count // GRID_W
    rows_all = rows_dev * lax.axis_size("sp")
    reach = NA_ROWS // 2
    lanes = bias_lanes(offset_bias)
    gains = lax.all_gather(norm_gain, "tp", axis=1, tiled=True).astype(jnp.float32)
    stream = residual
    for layer_index in range(LAYERS):
        full_float = lax.all_gather(stream, "tp", axis=1, tiled=True).astype(jnp.float32)
        inverse = lax.rsqrt(jnp.mean(full_float * full_float, axis=1, keepdims=True) + epsilon)
        normed = (full_float * inverse * gains[layer_index][None, :]).astype(jnp.bfloat16)
        keys = contract(normed, w_key[layer_index]).astype(jnp.bfloat16)
        values = contract(normed, w_value[layer_index]).astype(jnp.bfloat16)
        key_value = jnp.concatenate([keys, values], axis=1)
        padded = padded_2(key_value, (("sp", 0),), reach * GRID_W)
        queries = contract(normed, w_query[layer_index]).astype(jnp.bfloat16)
        queries = queries * jnp.bfloat16(HEAD_DIM ** (-0.5))
        attended = attention(queries, padded, lanes[layer_index], rows_dev, rows_all)
        gathered = lax.all_gather(attended, "tp", axis=1, tiled=True)
        mixed = contract(gathered, w_out[layer_index])
        stream = (stream.astype(jnp.float32) + mixed).astype(jnp.bfloat16)
    return stream


def per_device(residual, norm_gain, w_query, w_key, w_value, w_out, offset_bias):
    fits = offset_bias.shape[1] % 2 == 0 and 2 * HEAD_DIM == 128 and 2 * GRID_W == 128
    body = paired_device if fits else generic_device
    return body(residual, norm_gain, w_query, w_key, w_value, w_out, offset_bias)


def solution(mesh):
    in_specs = (
        P("sp", "tp"),
        P(None, "tp"),
        P(None, "tp", None),
        P(None, "tp", None),
        P(None, "tp", None),
        P(None, "tp", None),
        P(None, "tp", None, None),
    )
    out_specs = P("sp", "tp")
    return jax.shard_map(
        per_device, mesh=mesh, in_specs=in_specs, out_specs=out_specs, check_vma=False
    )
```

```python
import jax
import jax.numpy as jnp
from jax import lax
from jax.experimental import pallas as pl
from jax.experimental.pallas import tpu as pltpu
from jax.sharding import PartitionSpec as P

HEAD_DIM = 64
GRID_W = 64
NA_ROWS = 8
NA_COLS = 16
LAYERS = 3


epsilon = 1e-06


def padded_2(array, sides, width):
    for axis, dim in sides:
        size, length = (lax.axis_size(axis), array.shape[dim])
        up = [(i, (i + 1) % size) for i in range(size - 1)]
        down = [(j, i) for i, j in up]
        last = lax.slice_in_dim(array, length - width, length, axis=dim)
        first = lax.slice_in_dim(array, 0, width, axis=dim)
        before = lax.ppermute(last, axis, up)
        after = lax.ppermute(first, axis, down)
        array = jnp.concatenate([before, array, after], axis=dim)
    return array


def shortened(array):
    return jax.tree.map(lambda a: a.astype(jnp.bfloat16) if a.dtype == jnp.float32 else a, array)


def contract(left, right):
    return lax.dot_general(
        left, right, (((1,), (1,)), ((), ())), preferred_element_type=jnp.float32
    )


def generic_device(residual, norm_gain, w_query, w_key, w_value, w_out, offset_bias):
    token_count = residual.shape[0]
    local_feats = residual.shape[1]
    local_heads = offset_bias.shape[1]
    head_cols = local_heads * HEAD_DIM
    rows_dev = token_count // GRID_W
    rows_all = rows_dev * lax.axis_size("sp")
    row_base = lax.axis_index("sp") * rows_dev
    reach = NA_ROWS // 2
    slab_width = min(2 * NA_COLS, GRID_W)
    tile_starts = list(range(0, GRID_W, NA_COLS))
    slab_starts = [min(max(start - NA_COLS // 2, 0), GRID_W - slab_width) for start in tile_starts]
    tile_info = []
    for start, slab in zip(tile_starts, slab_starts):
        query_cols = start + jnp.arange(NA_COLS, dtype=jnp.int32)
        key_cols = slab + jnp.arange(slab_width, dtype=jnp.int32)
        first_col = jnp.clip(query_cols - NA_COLS // 2, 0, GRID_W - NA_COLS)
        inside = (key_cols[None, :] >= first_col[:, None]) & (
            key_cols[None, :] < first_col[:, None] + NA_COLS
        )
        offsets = key_cols[None, :] - query_cols[:, None] + (NA_COLS - 1)
        onehot = (offsets[:, :, None] == jnp.arange(2 * NA_COLS - 1, dtype=jnp.int32)).astype(
            jnp.float32
        )
        tile_info.append((start, slab, inside, onehot))
    stream = residual
    for layer_index in range(LAYERS):
        res_float = stream.astype(jnp.float32)
        gathered, gain_all = (
            lax.all_gather(stream, "tp", axis=1, tiled=True),
            lax.all_gather(norm_gain[layer_index][None, :], "tp", axis=1, tiled=True),
        )
        full_float = gathered.astype(jnp.float32)
        inverse = lax.rsqrt(jnp.mean(full_float * full_float, axis=1, keepdims=True) + epsilon)
        normed_all = (full_float * inverse * gain_all.astype(jnp.float32)).astype(jnp.bfloat16)
        queries = contract(normed_all, w_query[layer_index])
        keys = contract(normed_all, w_key[layer_index])
        values = contract(normed_all, w_value[layer_index])
        queries = queries.astype(jnp.bfloat16)
        key_value = jnp.concatenate(
            [keys.astype(jnp.bfloat16), values.astype(jnp.bfloat16)], axis=1
        )
        padded = padded_2(key_value, (("sp", 0),), reach * GRID_W)
        key_grid = padded.reshape(rows_dev + 2 * reach, GRID_W, 2, local_heads, HEAD_DIM)
        query_grid = queries.reshape(rows_dev, GRID_W, local_heads, HEAD_DIM)
        lookup = offset_bias[layer_index]

        def one_row(row_index, query_row):
            row_global = row_base + row_index
            first_row = jnp.clip(row_global - reach, 0, rows_all - NA_ROWS)
            local_first = first_row - row_base + reach
            window = lax.dynamic_slice_in_dim(key_grid, local_first, NA_ROWS, 0)
            row_offset = (
                first_row + jnp.arange(NA_ROWS, dtype=jnp.int32) - row_global + (NA_ROWS - 1)
            )
            row_onehot = (
                row_offset[:, None] == jnp.arange(2 * NA_ROWS - 1, dtype=jnp.int32)
            ).astype(jnp.float32)
            row_bias = jnp.einsum(
                "hab,ra->hrb", lookup, row_onehot, precision=lax.Precision.HIGHEST
            )
            pieces = []
            for start, slab, inside, onehot in tile_info:
                query_tile = query_row[start : start + NA_COLS]
                slab_keys = window[:, slab : slab + slab_width, 0]
                slab_values = window[:, slab : slab + slab_width, 1]
                bias_terms = jnp.einsum(
                    "hrb,wsb->hwrs", row_bias, onehot, precision=lax.Precision.HIGHEST
                )
                scores = jnp.einsum(
                    "whd,rshd->hwrs", query_tile, slab_keys, preferred_element_type=jnp.float32
                )
                scores = scores * HEAD_DIM ** (-0.5) + bias_terms
                scores = jnp.where(inside[None, :, None, :], scores, -jnp.inf)
                weights = jax.nn.softmax(
                    scores.reshape(local_heads, NA_COLS, NA_ROWS * slab_width), axis=-1
                ).astype(jnp.bfloat16)
                weights = weights.reshape(local_heads, NA_COLS, NA_ROWS, slab_width)
                attended = jnp.einsum(
                    "hwrs,rshd->whd", weights, slab_values, preferred_element_type=jnp.float32
                )
                pieces.append(attended.astype(jnp.bfloat16).reshape(NA_COLS, head_cols))
            return jnp.concatenate(pieces, axis=0)

        attended = jax.vmap(one_row)(jnp.arange(rows_dev, dtype=jnp.int32), query_grid).reshape(
            token_count, head_cols
        )
        portion = jax.tree.map(
            lambda part: lax.all_gather(part, "tp", axis=1, tiled=True), shortened(attended)
        )
        out_rows = lax.slice_in_dim(w_out[layer_index], 0, portion.shape[1], axis=1)
        mixed = jnp.zeros((token_count, local_feats), jnp.float32) + contract(portion, out_rows)
        stream = (res_float + mixed).astype(jnp.bfloat16)
    return stream


def bias_lanes(offset_bias):
    layers, heads, row_offs, col_offs = offset_bias.shape
    flipped = jnp.flip(offset_bias, axis=3)
    padded = jnp.pad(flipped, ((0, 0), (0, 0), (0, 1), (0, GRID_W - col_offs)))
    paired = padded.reshape(layers, heads // 2, 2, row_offs + 1, GRID_W)
    return paired.transpose(0, 1, 3, 2, 4).reshape(layers, heads // 2, row_offs + 1, 2 * GRID_W)


def window_mask():
    shape = (GRID_W, 2 * GRID_W)
    key_col = lax.broadcasted_iota(jnp.int32, shape, 0)
    query_col = lax.broadcasted_iota(jnp.int32, shape, 1) % GRID_W
    first = jnp.clip(query_col - NA_COLS // 2, 0, GRID_W - NA_COLS)
    return (key_col >= first) & (key_col < first + NA_COLS)


def build_table(lanes_of, table):
    inside = window_mask()
    for off in range(2 * NA_ROWS - 1):
        row = jnp.broadcast_to(lanes_of(off), (GRID_W, 2 * GRID_W))
        rolled = pltpu.roll(row, 2 * GRID_W - (NA_COLS - 1), axis=1, stride=1, stride_axis=0)
        table[off * GRID_W : (off + 1) * GRID_W, :] = jnp.where(inside, rolled, -1e30)


def attend_row(query, window_keys, window_values, bias):
    low = lax.broadcasted_iota(jnp.int32, query.shape, 1) < HEAD_DIM
    zero = jnp.zeros_like(query)
    block = jnp.concatenate([jnp.where(low, query, zero), jnp.where(low, zero, query)], axis=0)
    scores = contract(window_keys, block) + bias
    top = jnp.max(scores, axis=0, keepdims=True)
    weights = jnp.exp(scores - top)
    inverse = 1.0 / jnp.sum(weights, axis=0, keepdims=True)
    weights = (weights * inverse).astype(jnp.bfloat16)
    mixed = lax.dot_general(
        weights, window_values, (((0,), (0,)), ((), ())), preferred_element_type=jnp.float32
    )
    return jnp.where(low, mixed[:GRID_W], mixed[GRID_W:]).astype(jnp.bfloat16)


def row_window(row, rows_dev, rows_all):
    reach = NA_ROWS // 2
    row_base = lax.axis_index("sp") * rows_dev
    first = jnp.clip(row_base + row - reach, 0, rows_all - NA_ROWS)
    return first - row_base + reach, first - row_base - row + NA_ROWS - 1


MESH = pl.DeviceIdType.MESH


def tp_copy(src, dst, sems, index, peer):
    return pltpu.make_async_remote_copy(
        src_ref=src,
        dst_ref=dst,
        send_sem=sems.at[0, index],
        recv_sem=sems.at[1, index],
        device_id=(lax.axis_index("sp"), peer),
        device_id_type=MESH,
    )


class SquareGather:
    def __init__(self, slots, sems, chunks):
        self.slots, self.sems, self.chunks = slots, sems, chunks
        self.rows = slots.shape[1] // chunks
        self.me = lax.axis_index("tp")
        self.across = self.me + 1 - 2 * (self.me % 2)
        self.over = (self.me + 2) % 4
        self.corner = (self.across + 2) % 4

    def part(self, slot, chunk):
        start = chunk * self.rows
        if not isinstance(chunk, int):
            start = pl.multiple_of(start, self.rows)
        return self.slots.at[slot, pl.ds(start, self.rows), :]

    def copy(self, kind, slot, chunk, peer):
        part = self.part(slot, chunk)
        return tp_copy(part, part, self.sems.at[kind], chunk, peer)

    def send(self, chunk):
        self.copy(0, self.me, chunk, self.across).start()
        self.copy(1, self.me, chunk, self.over).start()

    def relay(self, chunk):
        self.copy(0, self.across, chunk, self.across).wait_recv()
        self.copy(1, self.over, chunk, self.over).wait_recv()

        @pl.when(chunk % 2 == 0)
        def _():
            self.copy(2, self.across, chunk, self.over).start()

        @pl.when(chunk % 2 == 1)
        def _():
            self.copy(2, self.over, chunk, self.across).start()

    def finish(self, chunk):
        self.copy(2, self.corner, chunk, self.over).wait_recv()

    def drain(self):
        def one(chunk, carry):
            self.copy(0, self.me, chunk, self.across).wait_send()
            self.copy(1, self.me, chunk, self.over).wait_send()
            self.copy(2, self.across, chunk, self.over).wait_send()
            return carry

        lax.fori_loop(0, self.chunks, one, 0)


def stack_kernel(
    rows_dev, rows_all,
    x_ref, gain_ref, lanes_ref, wq_ref, wk_ref, wv_ref, wo_ref, out_ref,
    gains, weights, stream, mixed, keyval, queries, normed, tables,
    weight_sems, gain_sems, stream_sems, mixed_sems, halo_sems,
):
    sp, sp_size = lax.axis_index("sp"), lax.axis_size("sp")
    layers = wq_ref.shape[0]
    tokens, feats = x_ref.shape
    width = feats
    reach = NA_ROWS // 2 * GRID_W
    streams = SquareGather(stream, stream_sems, rows_dev)
    mixes = SquareGather(mixed, mixed_sems, rows_dev)
    me, across, over = streams.me, streams.across, streams.over
    corner = streams.corner
    sources = (wk_ref, wv_ref, wq_ref, wo_ref)

    def weight_copy(kind, layer):
        return pltpu.make_async_copy(
            sources[kind].at[layer], weights.at[kind, layer], weight_sems.at[kind, layer]
        )

    for layer in range(layers):
        for kind in range(4):
            weight_copy(kind, layer).start()

    barrier = pltpu.get_barrier_semaphore()
    for peer in (across, over, corner):
        pl.semaphore_signal(barrier, inc=1, device_id=(sp, peer), device_id_type=MESH)

    @pl.when(sp > 0)
    def _():
        pl.semaphore_signal(barrier, inc=1, device_id=(sp - 1, me), device_id_type=MESH)

    @pl.when(sp < sp_size - 1)
    def _():
        pl.semaphore_signal(barrier, inc=1, device_id=(sp + 1, me), device_id_type=MESH)

    stream[me] = x_ref[...]
    gains[me] = gain_ref[...]
    sides = jnp.minimum(sp, 1) + jnp.minimum(sp_size - 1 - sp, 1)
    pl.semaphore_wait(barrier, 3 + sides)

    def gain_copy(index, slot, peer):
        return tp_copy(gains.at[slot], gains.at[slot], gain_sems, index, peer)

    for index, peer in enumerate((across, over, corner)):
        gain_copy(index, me, peer).start()
    for index, peer in enumerate((across, over, corner)):
        gain_copy(index, peer, peer).wait_recv()
        gain_copy(index, me, peer).wait_send()

    def halo_copy(parity, up):
        src = keyval.at[parity, pl.ds(tokens if up else reach, reach), :]
        dst = keyval.at[parity, pl.ds(0 if up else tokens + reach, reach), :]
        return pltpu.make_async_remote_copy(
            src_ref=src,
            dst_ref=dst,
            send_sem=halo_sems.at[0, parity, int(up)],
            recv_sem=halo_sems.at[1, parity, int(up)],
            device_id=(sp + 1 if up else sp - 1, me),
            device_id_type=MESH,
        )

    def one_layer(layer, carry):
        parity = layer % 2
        for chunk in range(rows_dev):
            streams.send(chunk)
        for pair in range(width // 128):
            build_table(
                lambda off: lanes_ref[layer, pair, off : off + 1, :], tables.at[pair]
            )

        def relay_chunk(chunk, carry):
            streams.relay(chunk)
            return carry

        lax.fori_loop(0, rows_dev, relay_chunk, 0)

        def norm_chunk(chunk, carry):
            streams.finish(chunk)
            here = pl.ds(pl.multiple_of(chunk * GRID_W, GRID_W), GRID_W)
            total = jnp.zeros((GRID_W, 1), jnp.float32)
            for slot in range(4):
                part = stream[slot, here, :].astype(jnp.float32)
                total += jnp.sum(part * part, axis=1, keepdims=True)
            inverse = lax.rsqrt(total * (1.0 / (4 * feats)) + epsilon)
            for slot in range(4):
                part = stream[slot, here, :].astype(jnp.float32)
                gain = gains[slot, pl.ds(layer, 1), :]
                normed[here, slot * feats : (slot + 1) * feats] = (
                    part * inverse * gain
                ).astype(jnp.bfloat16)
            return carry

        lax.fori_loop(0, rows_dev, norm_chunk, 0)
        streams.drain()
        for kind in range(2):
            weight_copy(kind, layer).wait()
            keyval[parity, reach : reach + tokens, kind * width : (kind + 1) * width] = contract(
                normed[...], weights[kind, layer]
            ).astype(jnp.bfloat16)

        @pl.when(sp > 0)
        def _():
            halo_copy(parity, False).start()

        @pl.when(sp < sp_size - 1)
        def _():
            halo_copy(parity, True).start()

        weight_copy(2, layer).wait()
        queries[...] = contract(normed[...], weights[2, layer]).astype(
            jnp.bfloat16
        ) * jnp.bfloat16(HEAD_DIM ** (-0.5))

        @pl.when(sp > 0)
        def _():
            halo_copy(parity, True).wait_recv()

        @pl.when(sp < sp_size - 1)
        def _():
            halo_copy(parity, False).wait_recv()

        def one_row(row, carry):
            start, off = row_window(row, rows_dev, rows_all)
            keys = pl.ds(pl.multiple_of(start * GRID_W, GRID_W), NA_ROWS * GRID_W)
            here = pl.ds(pl.multiple_of(row * GRID_W, GRID_W), GRID_W)
            offs = pl.ds(pl.multiple_of(off * GRID_W, GRID_W), NA_ROWS * GRID_W)
            for pair in range(width // 128):
                cols = slice(pair * 128, (pair + 1) * 128)
                vcols = slice(width + pair * 128, width + (pair + 1) * 128)
                mixed[me, here, cols] = attend_row(
                    queries[here, cols],
                    keyval[parity, keys, cols],
                    keyval[parity, keys, vcols],
                    tables[pair, offs, :],
                )
            mixes.send(row)

            @pl.when(row > 0)
            def _():
                mixes.relay(row - 1)

            return carry

        lax.fori_loop(0, rows_dev, one_row, 0)
        mixes.relay(rows_dev - 1)

        @pl.when(sp > 0)
        def _():
            halo_copy(parity, False).wait_send()

        @pl.when(sp < sp_size - 1)
        def _():
            halo_copy(parity, True).wait_send()

        def finish_chunk(chunk, carry):
            mixes.finish(chunk)
            return carry

        lax.fori_loop(0, rows_dev, finish_chunk, 0)
        mixes.drain()
        weight_copy(3, layer).wait()
        total = stream[me].astype(jnp.float32)
        for slot in range(4):
            total += contract(
                mixed[slot], weights[3, layer, :, slot * width : (slot + 1) * width]
            )
        stream[me] = total.astype(jnp.bfloat16)
        return carry

    lax.fori_loop(0, layers, one_layer, 0)
    out_ref[...] = stream[me]


def square_device(residual, norm_gain, w_query, w_key, w_value, w_out, offset_bias):
    tokens, feats = residual.shape
    layers = w_query.shape[0]
    rows_dev = tokens // GRID_W
    rows_all = rows_dev * lax.axis_size("sp")
    lanes = bias_lanes(offset_bias)
    gain = jnp.pad(norm_gain.astype(jnp.float32), ((0, 8 - layers), (0, 0)))
    vmem = pl.BlockSpec(memory_space=pltpu.VMEM)
    hbm = pl.BlockSpec(memory_space=pl.ANY)
    bf16, dma = jnp.bfloat16, pltpu.SemaphoreType.DMA
    padded = tokens + NA_ROWS * GRID_W
    return pl.pallas_call(
        lambda *refs: stack_kernel(rows_dev, rows_all, *refs),
        out_shape=jax.ShapeDtypeStruct(residual.shape, bf16),
        in_specs=[vmem] * 3 + [hbm] * 4,
        out_specs=vmem,
        scratch_shapes=[
            pltpu.VMEM((4, 8, feats), jnp.float32),
            pltpu.VMEM((4,) + w_query.shape, bf16),
            pltpu.VMEM((4, tokens, feats), bf16),
            pltpu.VMEM((4, tokens, feats), bf16),
            pltpu.VMEM((2, padded, 2 * feats), bf16),
            pltpu.VMEM((tokens, feats), bf16),
            pltpu.VMEM((tokens, 4 * feats), bf16),
            pltpu.VMEM((feats // 128, (2 * NA_ROWS - 1) * GRID_W, 128), jnp.float32),
            dma((4, layers)),
            dma((2, 3)),
            dma((3, 2, rows_dev)),
            dma((3, 2, rows_dev)),
            dma((2, 2, 2)),
        ],
        compiler_params=pltpu.CompilerParams(
            collective_id=0, has_side_effects=True, vmem_limit_bytes=56 * 1024 * 1024
        ),
        name="stack",
    )(residual, gain, lanes, w_query, w_key, w_value, w_out)


def per_device(residual, norm_gain, w_query, w_key, w_value, w_out, offset_bias):
    paired = offset_bias.shape[1] % 2 == 0 and 2 * HEAD_DIM == 128 and 2 * GRID_W == 128
    square = lax.axis_size("tp") == 4 and offset_bias.shape[1] * HEAD_DIM == residual.shape[1]
    body = generic_device
    if paired and square:
        body = square_device
    return body(residual, norm_gain, w_query, w_key, w_value, w_out, offset_bias)


def solution(mesh):
    in_specs = (
        P("sp", "tp"),
        P(None, "tp"),
        P(None, "tp", None),
        P(None, "tp", None),
        P(None, "tp", None),
        P(None, "tp", None),
        P(None, "tp", None, None),
    )
    out_specs = P("sp", "tp")
    return jax.shard_map(
        per_device, mesh=mesh, in_specs=in_specs, out_specs=out_specs, check_vma=False
    )
```

```python
import jax
import jax.numpy as jnp
from jax import lax
from jax.experimental import pallas as pl
from jax.experimental.pallas import tpu as pltpu
from jax.sharding import PartitionSpec as P

HEAD_DIM = 64
GRID_W = 64
NA_ROWS = 8
NA_COLS = 16
LAYERS = 3


epsilon = 1e-06


def padded_2(array, sides, width):
    for axis, dim in sides:
        size, length = (lax.axis_size(axis), array.shape[dim])
        up = [(i, (i + 1) % size) for i in range(size - 1)]
        down = [(j, i) for i, j in up]
        last = lax.slice_in_dim(array, length - width, length, axis=dim)
        first = lax.slice_in_dim(array, 0, width, axis=dim)
        before = lax.ppermute(last, axis, up)
        after = lax.ppermute(first, axis, down)
        array = jnp.concatenate([before, array, after], axis=dim)
    return array


def shortened(array):
    return jax.tree.map(lambda a: a.astype(jnp.bfloat16) if a.dtype == jnp.float32 else a, array)


def contract(left, right):
    return lax.dot_general(
        left, right, (((1,), (1,)), ((), ())), preferred_element_type=jnp.float32
    )


def generic_device(residual, norm_gain, w_query, w_key, w_value, w_out, offset_bias):
    token_count = residual.shape[0]
    local_feats = residual.shape[1]
    local_heads = offset_bias.shape[1]
    head_cols = local_heads * HEAD_DIM
    rows_dev = token_count // GRID_W
    rows_all = rows_dev * lax.axis_size("sp")
    row_base = lax.axis_index("sp") * rows_dev
    reach = NA_ROWS // 2
    slab_width = min(2 * NA_COLS, GRID_W)
    tile_starts = list(range(0, GRID_W, NA_COLS))
    slab_starts = [min(max(start - NA_COLS // 2, 0), GRID_W - slab_width) for start in tile_starts]
    tile_info = []
    for start, slab in zip(tile_starts, slab_starts):
        query_cols = start + jnp.arange(NA_COLS, dtype=jnp.int32)
        key_cols = slab + jnp.arange(slab_width, dtype=jnp.int32)
        first_col = jnp.clip(query_cols - NA_COLS // 2, 0, GRID_W - NA_COLS)
        inside = (key_cols[None, :] >= first_col[:, None]) & (
            key_cols[None, :] < first_col[:, None] + NA_COLS
        )
        offsets = key_cols[None, :] - query_cols[:, None] + (NA_COLS - 1)
        onehot = (offsets[:, :, None] == jnp.arange(2 * NA_COLS - 1, dtype=jnp.int32)).astype(
            jnp.float32
        )
        tile_info.append((start, slab, inside, onehot))
    stream = residual
    for layer_index in range(LAYERS):
        res_float = stream.astype(jnp.float32)
        gathered, gain_all = (
            lax.all_gather(stream, "tp", axis=1, tiled=True),
            lax.all_gather(norm_gain[layer_index][None, :], "tp", axis=1, tiled=True),
        )
        full_float = gathered.astype(jnp.float32)
        inverse = lax.rsqrt(jnp.mean(full_float * full_float, axis=1, keepdims=True) + epsilon)
        normed_all = (full_float * inverse * gain_all.astype(jnp.float32)).astype(jnp.bfloat16)
        queries = contract(normed_all, w_query[layer_index])
        keys = contract(normed_all, w_key[layer_index])
        values = contract(normed_all, w_value[layer_index])
        queries = queries.astype(jnp.bfloat16)
        key_value = jnp.concatenate(
            [keys.astype(jnp.bfloat16), values.astype(jnp.bfloat16)], axis=1
        )
        padded = padded_2(key_value, (("sp", 0),), reach * GRID_W)
        key_grid = padded.reshape(rows_dev + 2 * reach, GRID_W, 2, local_heads, HEAD_DIM)
        query_grid = queries.reshape(rows_dev, GRID_W, local_heads, HEAD_DIM)
        lookup = offset_bias[layer_index]

        def one_row(row_index, query_row):
            row_global = row_base + row_index
            first_row = jnp.clip(row_global - reach, 0, rows_all - NA_ROWS)
            local_first = first_row - row_base + reach
            window = lax.dynamic_slice_in_dim(key_grid, local_first, NA_ROWS, 0)
            row_offset = (
                first_row + jnp.arange(NA_ROWS, dtype=jnp.int32) - row_global + (NA_ROWS - 1)
            )
            row_onehot = (
                row_offset[:, None] == jnp.arange(2 * NA_ROWS - 1, dtype=jnp.int32)
            ).astype(jnp.float32)
            row_bias = jnp.einsum(
                "hab,ra->hrb", lookup, row_onehot, precision=lax.Precision.HIGHEST
            )
            pieces = []
            for start, slab, inside, onehot in tile_info:
                query_tile = query_row[start : start + NA_COLS]
                slab_keys = window[:, slab : slab + slab_width, 0]
                slab_values = window[:, slab : slab + slab_width, 1]
                bias_terms = jnp.einsum(
                    "hrb,wsb->hwrs", row_bias, onehot, precision=lax.Precision.HIGHEST
                )
                scores = jnp.einsum(
                    "whd,rshd->hwrs", query_tile, slab_keys, preferred_element_type=jnp.float32
                )
                scores = scores * HEAD_DIM ** (-0.5) + bias_terms
                scores = jnp.where(inside[None, :, None, :], scores, -jnp.inf)
                weights = jax.nn.softmax(
                    scores.reshape(local_heads, NA_COLS, NA_ROWS * slab_width), axis=-1
                ).astype(jnp.bfloat16)
                weights = weights.reshape(local_heads, NA_COLS, NA_ROWS, slab_width)
                attended = jnp.einsum(
                    "hwrs,rshd->whd", weights, slab_values, preferred_element_type=jnp.float32
                )
                pieces.append(attended.astype(jnp.bfloat16).reshape(NA_COLS, head_cols))
            return jnp.concatenate(pieces, axis=0)

        attended = jax.vmap(one_row)(jnp.arange(rows_dev, dtype=jnp.int32), query_grid).reshape(
            token_count, head_cols
        )
        portion = jax.tree.map(
            lambda part: lax.all_gather(part, "tp", axis=1, tiled=True), shortened(attended)
        )
        out_rows = lax.slice_in_dim(w_out[layer_index], 0, portion.shape[1], axis=1)
        mixed = jnp.zeros((token_count, local_feats), jnp.float32) + contract(portion, out_rows)
        stream = (res_float + mixed).astype(jnp.bfloat16)
    return stream


def bias_lanes(offset_bias):
    layers, heads, row_offs, col_offs = offset_bias.shape
    flipped = jnp.flip(offset_bias, axis=3)
    padded = jnp.pad(flipped, ((0, 0), (0, 0), (0, 1), (0, GRID_W - col_offs)))
    paired = padded.reshape(layers, heads // 2, 2, row_offs + 1, GRID_W)
    return paired.transpose(0, 1, 3, 2, 4).reshape(layers, heads // 2, row_offs + 1, 2 * GRID_W)


def window_mask():
    shape = (GRID_W, 2 * GRID_W)
    key_col = lax.broadcasted_iota(jnp.int32, shape, 0)
    query_col = lax.broadcasted_iota(jnp.int32, shape, 1) % GRID_W
    first = jnp.clip(query_col - NA_COLS // 2, 0, GRID_W - NA_COLS)
    return (key_col >= first) & (key_col < first + NA_COLS)


def build_table(lanes_of, table):
    inside = window_mask()
    for off in range(2 * NA_ROWS - 1):
        row = jnp.broadcast_to(lanes_of(off), (GRID_W, 2 * GRID_W))
        rolled = pltpu.roll(row, 2 * GRID_W - (NA_COLS - 1), axis=1, stride=1, stride_axis=0)
        table[off * GRID_W : (off + 1) * GRID_W, :] = jnp.where(inside, rolled, -1e30)


def attend_row(query, window_keys, window_values, bias):
    low = lax.broadcasted_iota(jnp.int32, query.shape, 1) < HEAD_DIM
    zero = jnp.zeros_like(query)
    block = jnp.concatenate([jnp.where(low, query, zero), jnp.where(low, zero, query)], axis=0)
    scores = contract(window_keys, block) + bias
    top = jnp.max(scores, axis=0, keepdims=True)
    weights = jnp.exp(scores - top)
    inverse = 1.0 / jnp.sum(weights, axis=0, keepdims=True)
    weights = (weights * inverse).astype(jnp.bfloat16)
    mixed = lax.dot_general(
        weights, window_values, (((0,), (0,)), ((), ())), preferred_element_type=jnp.float32
    )
    return jnp.where(low, mixed[:GRID_W], mixed[GRID_W:]).astype(jnp.bfloat16)


def row_window(row, rows_dev, rows_all):
    reach = NA_ROWS // 2
    row_base = lax.axis_index("sp") * rows_dev
    first = jnp.clip(row_base + row - reach, 0, rows_all - NA_ROWS)
    return first - row_base + reach, first - row_base - row + NA_ROWS - 1


MESH = pl.DeviceIdType.MESH
LAG = 3


def tp_copy(src, dst, sems, index, peer):
    return pltpu.make_async_remote_copy(
        src_ref=src,
        dst_ref=dst,
        send_sem=sems.at[0, index],
        recv_sem=sems.at[1, index],
        device_id=(lax.axis_index("sp"), peer),
        device_id_type=MESH,
    )


class SquareGather:
    def __init__(self, slots, sems, chunks):
        self.slots, self.sems, self.chunks = slots, sems, chunks
        self.rows = slots.shape[1] // chunks
        self.me = lax.axis_index("tp")
        self.across = self.me + 1 - 2 * (self.me % 2)
        self.over = (self.me + 2) % 4
        self.corner = (self.across + 2) % 4

    def part(self, slot, chunk):
        start = chunk * self.rows
        if not isinstance(chunk, int):
            start = pl.multiple_of(start, self.rows)
        return self.slots.at[slot, pl.ds(start, self.rows), :]

    def copy(self, kind, slot, chunk, peer):
        part = self.part(slot, chunk)
        return tp_copy(part, part, self.sems.at[kind], chunk, peer)

    def send(self, chunk):
        self.copy(0, self.me, chunk, self.across).start()
        self.copy(1, self.me, chunk, self.over).start()

    def relay(self, chunk):
        self.copy(0, self.across, chunk, self.across).wait_recv()
        self.copy(1, self.over, chunk, self.over).wait_recv()

        @pl.when(chunk % 2 == 0)
        def _():
            self.copy(2, self.across, chunk, self.over).start()

        @pl.when(chunk % 2 == 1)
        def _():
            self.copy(2, self.over, chunk, self.across).start()

    def finish(self, chunk):
        self.copy(2, self.corner, chunk, self.over).wait_recv()

    def drain(self):
        def one(chunk, carry):
            self.copy(0, self.me, chunk, self.across).wait_send()
            self.copy(1, self.me, chunk, self.over).wait_send()
            self.copy(2, self.across, chunk, self.over).wait_send()
            return carry

        lax.fori_loop(0, self.chunks, one, 0)


def stack_kernel(
    rows_dev, rows_all,
    x_ref, gain_ref, lanes_ref, wq_ref, wk_ref, wv_ref, wo_ref, out_ref,
    gains, weights, stream, mixed, keyval, queries, normed, tables,
    partial, weight_sems, gain_sems, stream_sems, mixed_sems, halo_sems,
):
    sp, sp_size = lax.axis_index("sp"), lax.axis_size("sp")
    layers = wq_ref.shape[0]
    tokens, feats = x_ref.shape
    width = feats
    reach = NA_ROWS // 2 * GRID_W
    streams = SquareGather(stream, stream_sems, rows_dev)
    mixes = SquareGather(mixed, mixed_sems, rows_dev)
    me, across, over = streams.me, streams.across, streams.over
    corner = streams.corner
    sources = (wk_ref, wv_ref, wq_ref, wo_ref)

    def weight_copy(kind, layer):
        return pltpu.make_async_copy(
            sources[kind].at[layer], weights.at[kind, layer], weight_sems.at[kind, layer]
        )

    for layer in range(layers):
        for kind in range(4):
            weight_copy(kind, layer).start()

    barrier = pltpu.get_barrier_semaphore()
    for peer in (across, over, corner):
        pl.semaphore_signal(barrier, inc=1, device_id=(sp, peer), device_id_type=MESH)

    @pl.when(sp > 0)
    def _():
        pl.semaphore_signal(barrier, inc=1, device_id=(sp - 1, me), device_id_type=MESH)

    @pl.when(sp < sp_size - 1)
    def _():
        pl.semaphore_signal(barrier, inc=1, device_id=(sp + 1, me), device_id_type=MESH)

    stream[me] = x_ref[...]
    gains[me, 0:layers, :] = gain_ref[...].astype(jnp.float32)
    sides = jnp.minimum(sp, 1) + jnp.minimum(sp_size - 1 - sp, 1)
    pl.semaphore_wait(barrier, 3 + sides)

    def gain_copy(index, slot, peer):
        return tp_copy(gains.at[slot], gains.at[slot], gain_sems, index, peer)

    for index, peer in enumerate((across, over, corner)):
        gain_copy(index, me, peer).start()

    pairs = rows_dev // 2
    tall = 2 * GRID_W
    parts = NA_ROWS // 4
    down_parts = range(parts)
    up_parts = range(pairs - parts, pairs)
    order = sorted(range(pairs), key=lambda j: -((j in down_parts) + (j in up_parts)))

    def halo_copy(parity, up, part, kind):
        cols = slice(kind * width, (kind + 1) * width)
        local = reach + (pairs - parts + part if up else part) * tall
        there = part * tall + (0 if up else tokens + reach)
        return pltpu.make_async_remote_copy(
            src_ref=keyval.at[parity, pl.ds(local, tall), cols],
            dst_ref=keyval.at[parity, pl.ds(there, tall), cols],
            send_sem=halo_sems.at[0, parity, int(up), part, kind],
            recv_sem=halo_sems.at[1, parity, int(up), part, kind],
            device_id=(sp + 1 if up else sp - 1, me),
            device_id_type=MESH,
        )

    def send_halo(parity, pair, kind):
        if pair in down_parts:

            @pl.when(sp > 0)
            def _():
                halo_copy(parity, False, pair, kind).start()

        if pair in up_parts:

            @pl.when(sp < sp_size - 1)
            def _():
                halo_copy(parity, True, pair - (pairs - parts), kind).start()

    def one_layer(layer, carry):
        parity = layer % 2
        for pair in order[:2]:
            streams.send(2 * pair)
            streams.send(2 * pair + 1)
        for pair in range(width // 128):
            build_table(
                lambda off: lanes_ref[layer, pair, off : off + 1, :], tables.at[pair]
            )

        def relay_pair(pair):
            streams.relay(2 * pair)
            streams.relay(2 * pair + 1)

        def norm_pair(pair):
            here = slice(pair * tall, (pair + 1) * tall)
            total = jnp.zeros((tall, 1), jnp.float32)
            for slot in range(4):
                part = stream[slot, here, :].astype(jnp.float32)
                total += jnp.sum(part * part, axis=1, keepdims=True)
            inverse = lax.rsqrt(total * (1.0 / (4 * feats)) + epsilon)
            for slot in range(4):
                part = stream[slot, here, :].astype(jnp.float32)
                gain = gains[slot, pl.ds(layer, 1), :]
                normed[here, slot * feats : (slot + 1) * feats] = (
                    part * inverse * gain
                ).astype(jnp.bfloat16)

        def project_pair(pair):
            here = slice(pair * tall, (pair + 1) * tall)
            there = slice(reach + pair * tall, reach + (pair + 1) * tall)
            for kind in range(2):
                keyval[parity, there, kind * width : (kind + 1) * width] = contract(
                    normed[here, :], weights[kind, layer]
                ).astype(jnp.bfloat16)
                send_halo(parity, pair, kind)
            queries[here, :] = contract(normed[here, :], weights[2, layer]).astype(
                jnp.bfloat16
            ) * jnp.bfloat16(HEAD_DIM ** (-0.5))

        @pl.when(layer == 0)
        def _():
            for index, peer in enumerate((across, over, corner)):
                gain_copy(index, peer, peer).wait_recv()
                gain_copy(index, me, peer).wait_send()

        for kind in range(3):
            weight_copy(kind, layer).wait()
        relay_pair(order[0])
        for pair in order[2:]:
            streams.send(2 * pair)
            streams.send(2 * pair + 1)
        for place, pair in enumerate(order):
            if place + 1 < pairs:
                relay_pair(order[place + 1])
            streams.finish(2 * pair)
            streams.finish(2 * pair + 1)
            norm_pair(pair)
            project_pair(pair)
        streams.drain()

        for part in range(parts):
            for kind in range(2):

                @pl.when(sp > 0)
                def _():
                    halo_copy(parity, True, part, kind).wait_recv()

                @pl.when(sp < sp_size - 1)
                def _():
                    halo_copy(parity, False, part, kind).wait_recv()

        def one_row(row, carry):
            start, off = row_window(row, rows_dev, rows_all)
            keys = pl.ds(pl.multiple_of(start * GRID_W, GRID_W), NA_ROWS * GRID_W)
            here = pl.ds(pl.multiple_of(row * GRID_W, GRID_W), GRID_W)
            offs = pl.ds(pl.multiple_of(off * GRID_W, GRID_W), NA_ROWS * GRID_W)
            for pair in range(width // 128):
                cols = slice(pair * 128, (pair + 1) * 128)
                vcols = slice(width + pair * 128, width + (pair + 1) * 128)
                mixed[me, here, cols] = attend_row(
                    queries[here, cols],
                    keyval[parity, keys, cols],
                    keyval[parity, keys, vcols],
                    tables[pair, offs, :],
                )
            mixes.send(row)

            @pl.when(row >= LAG)
            def _():
                mixes.relay(row - LAG)

            return carry

        lax.fori_loop(0, rows_dev, one_row, 0)

        def relay_rest(row, carry):
            mixes.relay(row)
            return carry

        lax.fori_loop(rows_dev - LAG, rows_dev, relay_rest, 0)
        weight_copy(3, layer).wait()

        def out_part(slot):
            cols = pl.ds(pl.multiple_of(slot * width, width), width)
            return contract(mixed[slot], weights[3, layer, :, cols])

        total = stream[me].astype(jnp.float32) + out_part(me)
        partial[...] = total + out_part(across) + out_part(over)

        for part in range(parts):
            for kind in range(2):

                @pl.when(sp > 0)
                def _():
                    halo_copy(parity, False, part, kind).wait_send()

                @pl.when(sp < sp_size - 1)
                def _():
                    halo_copy(parity, True, part, kind).wait_send()

        def finish_chunk(chunk, carry):
            mixes.finish(chunk)
            return carry

        lax.fori_loop(0, rows_dev, finish_chunk, 0)
        mixes.drain()
        total = partial[...] + out_part(corner)
        stream[me] = total.astype(jnp.bfloat16)
        return carry

    lax.fori_loop(0, layers, one_layer, 0)
    out_ref[...] = stream[me]


def square_device(residual, norm_gain, w_query, w_key, w_value, w_out, offset_bias):
    tokens, feats = residual.shape
    layers = w_query.shape[0]
    rows_dev = tokens // GRID_W
    rows_all = rows_dev * lax.axis_size("sp")
    lanes = bias_lanes(offset_bias)
    vmem = pl.BlockSpec(memory_space=pltpu.VMEM)
    hbm = pl.BlockSpec(memory_space=pl.ANY)
    bf16, dma = jnp.bfloat16, pltpu.SemaphoreType.DMA
    padded = tokens + NA_ROWS * GRID_W
    return pl.pallas_call(
        lambda *refs: stack_kernel(rows_dev, rows_all, *refs),
        out_shape=jax.ShapeDtypeStruct(residual.shape, bf16),
        in_specs=[vmem] * 3 + [hbm] * 4,
        out_specs=vmem,
        scratch_shapes=[
            pltpu.VMEM((4, -(-layers // 8) * 8, feats), jnp.float32),
            pltpu.VMEM((4,) + w_query.shape, bf16),
            pltpu.VMEM((4, tokens, feats), bf16),
            pltpu.VMEM((4, tokens, feats), bf16),
            pltpu.VMEM((2, padded, 2 * feats), bf16),
            pltpu.VMEM((tokens, feats), bf16),
            pltpu.VMEM((tokens, 4 * feats), bf16),
            pltpu.VMEM((feats // 128, (2 * NA_ROWS - 1) * GRID_W, 128), jnp.float32),
            pltpu.VMEM((tokens, feats), jnp.float32),
            dma((4, layers)),
            dma((2, 3)),
            dma((3, 2, rows_dev)),
            dma((3, 2, rows_dev)),
            dma((2, 2, 2, NA_ROWS // 4, 2)),
        ],
        compiler_params=pltpu.CompilerParams(
            collective_id=0, has_side_effects=True, vmem_limit_bytes=56 * 1024 * 1024
        ),
        name="stack",
    )(residual, norm_gain, lanes, w_query, w_key, w_value, w_out)


def per_device(residual, norm_gain, w_query, w_key, w_value, w_out, offset_bias):
    paired = offset_bias.shape[1] % 2 == 0 and 2 * HEAD_DIM == 128 and 2 * GRID_W == 128
    square = lax.axis_size("tp") == 4 and offset_bias.shape[1] * HEAD_DIM == residual.shape[1]
    rows_dev = residual.shape[0] // GRID_W
    even = rows_dev % 2 == 0 and rows_dev >= NA_ROWS // 2
    body = generic_device
    if paired and square and even:
        body = square_device
    return body(residual, norm_gain, w_query, w_key, w_value, w_out, offset_bias)


def solution(mesh):
    in_specs = (
        P("sp", "tp"),
        P(None, "tp"),
        P(None, "tp", None),
        P(None, "tp", None),
        P(None, "tp", None),
        P(None, "tp", None),
        P(None, "tp", None, None),
    )
    out_specs = P("sp", "tp")
    return jax.shard_map(
        per_device, mesh=mesh, in_specs=in_specs, out_specs=out_specs, check_vma=False
    )
```

```python
import jax
import jax.numpy as jnp
from jax import lax
from jax.experimental import pallas as pl
from jax.experimental.pallas import tpu as pltpu
from jax.sharding import PartitionSpec as P

HEAD_DIM = 64
GRID_W = 64
NA_ROWS = 8
NA_COLS = 16
LAYERS = 3


epsilon = 1e-06


def padded_2(array, sides, width):
    for axis, dim in sides:
        size, length = (lax.axis_size(axis), array.shape[dim])
        up = [(i, (i + 1) % size) for i in range(size - 1)]
        down = [(j, i) for i, j in up]
        last = lax.slice_in_dim(array, length - width, length, axis=dim)
        first = lax.slice_in_dim(array, 0, width, axis=dim)
        before = lax.ppermute(last, axis, up)
        after = lax.ppermute(first, axis, down)
        array = jnp.concatenate([before, array, after], axis=dim)
    return array


def shortened(array):
    return jax.tree.map(lambda a: a.astype(jnp.bfloat16) if a.dtype == jnp.float32 else a, array)


def contract(left, right):
    return lax.dot_general(
        left, right, (((1,), (1,)), ((), ())), preferred_element_type=jnp.float32
    )


def generic_device(residual, norm_gain, w_query, w_key, w_value, w_out, offset_bias):
    token_count = residual.shape[0]
    local_feats = residual.shape[1]
    local_heads = offset_bias.shape[1]
    head_cols = local_heads * HEAD_DIM
    rows_dev = token_count // GRID_W
    rows_all = rows_dev * lax.axis_size("sp")
    row_base = lax.axis_index("sp") * rows_dev
    reach = NA_ROWS // 2
    slab_width = min(2 * NA_COLS, GRID_W)
    tile_starts = list(range(0, GRID_W, NA_COLS))
    slab_starts = [min(max(start - NA_COLS // 2, 0), GRID_W - slab_width) for start in tile_starts]
    tile_info = []
    for start, slab in zip(tile_starts, slab_starts):
        query_cols = start + jnp.arange(NA_COLS, dtype=jnp.int32)
        key_cols = slab + jnp.arange(slab_width, dtype=jnp.int32)
        first_col = jnp.clip(query_cols - NA_COLS // 2, 0, GRID_W - NA_COLS)
        inside = (key_cols[None, :] >= first_col[:, None]) & (
            key_cols[None, :] < first_col[:, None] + NA_COLS
        )
        offsets = key_cols[None, :] - query_cols[:, None] + (NA_COLS - 1)
        onehot = (offsets[:, :, None] == jnp.arange(2 * NA_COLS - 1, dtype=jnp.int32)).astype(
            jnp.float32
        )
        tile_info.append((start, slab, inside, onehot))
    stream = residual
    for layer_index in range(LAYERS):
        res_float = stream.astype(jnp.float32)
        gathered, gain_all = (
            lax.all_gather(stream, "tp", axis=1, tiled=True),
            lax.all_gather(norm_gain[layer_index][None, :], "tp", axis=1, tiled=True),
        )
        full_float = gathered.astype(jnp.float32)
        inverse = lax.rsqrt(jnp.mean(full_float * full_float, axis=1, keepdims=True) + epsilon)
        normed_all = (full_float * inverse * gain_all.astype(jnp.float32)).astype(jnp.bfloat16)
        queries = contract(normed_all, w_query[layer_index])
        keys = contract(normed_all, w_key[layer_index])
        values = contract(normed_all, w_value[layer_index])
        queries = queries.astype(jnp.bfloat16)
        key_value = jnp.concatenate(
            [keys.astype(jnp.bfloat16), values.astype(jnp.bfloat16)], axis=1
        )
        padded = padded_2(key_value, (("sp", 0),), reach * GRID_W)
        key_grid = padded.reshape(rows_dev + 2 * reach, GRID_W, 2, local_heads, HEAD_DIM)
        query_grid = queries.reshape(rows_dev, GRID_W, local_heads, HEAD_DIM)
        lookup = offset_bias[layer_index]

        def one_row(row_index, query_row):
            row_global = row_base + row_index
            first_row = jnp.clip(row_global - reach, 0, rows_all - NA_ROWS)
            local_first = first_row - row_base + reach
            window = lax.dynamic_slice_in_dim(key_grid, local_first, NA_ROWS, 0)
            row_offset = (
                first_row + jnp.arange(NA_ROWS, dtype=jnp.int32) - row_global + (NA_ROWS - 1)
            )
            row_onehot = (
                row_offset[:, None] == jnp.arange(2 * NA_ROWS - 1, dtype=jnp.int32)
            ).astype(jnp.float32)
            row_bias = jnp.einsum(
                "hab,ra->hrb", lookup, row_onehot, precision=lax.Precision.HIGHEST
            )
            pieces = []
            for start, slab, inside, onehot in tile_info:
                query_tile = query_row[start : start + NA_COLS]
                slab_keys = window[:, slab : slab + slab_width, 0]
                slab_values = window[:, slab : slab + slab_width, 1]
                bias_terms = jnp.einsum(
                    "hrb,wsb->hwrs", row_bias, onehot, precision=lax.Precision.HIGHEST
                )
                scores = jnp.einsum(
                    "whd,rshd->hwrs", query_tile, slab_keys, preferred_element_type=jnp.float32
                )
                scores = scores * HEAD_DIM ** (-0.5) + bias_terms
                scores = jnp.where(inside[None, :, None, :], scores, -jnp.inf)
                weights = jax.nn.softmax(
                    scores.reshape(local_heads, NA_COLS, NA_ROWS * slab_width), axis=-1
                ).astype(jnp.bfloat16)
                weights = weights.reshape(local_heads, NA_COLS, NA_ROWS, slab_width)
                attended = jnp.einsum(
                    "hwrs,rshd->whd", weights, slab_values, preferred_element_type=jnp.float32
                )
                pieces.append(attended.astype(jnp.bfloat16).reshape(NA_COLS, head_cols))
            return jnp.concatenate(pieces, axis=0)

        attended = jax.vmap(one_row)(jnp.arange(rows_dev, dtype=jnp.int32), query_grid).reshape(
            token_count, head_cols
        )
        portion = jax.tree.map(
            lambda part: lax.all_gather(part, "tp", axis=1, tiled=True), shortened(attended)
        )
        out_rows = lax.slice_in_dim(w_out[layer_index], 0, portion.shape[1], axis=1)
        mixed = jnp.zeros((token_count, local_feats), jnp.float32) + contract(portion, out_rows)
        stream = (res_float + mixed).astype(jnp.bfloat16)
    return stream


def bias_lanes(offset_bias):
    layers, heads, row_offs, col_offs = offset_bias.shape
    flipped = jnp.flip(offset_bias, axis=3)
    padded = jnp.pad(flipped, ((0, 0), (0, 0), (0, 1), (0, GRID_W - col_offs)))
    paired = padded.reshape(layers, heads // 2, 2, row_offs + 1, GRID_W)
    return paired.transpose(0, 1, 3, 2, 4).reshape(layers, heads // 2, row_offs + 1, 2 * GRID_W)


def window_mask():
    shape = (GRID_W, 2 * GRID_W)
    key_col = lax.broadcasted_iota(jnp.int32, shape, 0)
    query_col = lax.broadcasted_iota(jnp.int32, shape, 1) % GRID_W
    first = jnp.clip(query_col - NA_COLS // 2, 0, GRID_W - NA_COLS)
    return (key_col >= first) & (key_col < first + NA_COLS)


def build_table(lanes_of, table):
    inside = window_mask()
    for off in range(2 * NA_ROWS - 1):
        row = jnp.broadcast_to(lanes_of(off), (GRID_W, 2 * GRID_W))
        rolled = pltpu.roll(row, 2 * GRID_W - (NA_COLS - 1), axis=1, stride=1, stride_axis=0)
        table[off * GRID_W : (off + 1) * GRID_W, :] = jnp.where(inside, rolled, -1e30)


def attend_row(query, window_keys, window_values, bias):
    low = lax.broadcasted_iota(jnp.int32, query.shape, 1) < HEAD_DIM
    zero = jnp.zeros_like(query)
    block = jnp.concatenate([jnp.where(low, query, zero), jnp.where(low, zero, query)], axis=0)
    scores = contract(window_keys, block) + bias
    top = jnp.max(scores, axis=0, keepdims=True)
    weights = jnp.exp(scores - top)
    inverse = 1.0 / jnp.sum(weights, axis=0, keepdims=True)
    weights = (weights * inverse).astype(jnp.bfloat16)
    mixed = lax.dot_general(
        weights, window_values, (((0,), (0,)), ((), ())), preferred_element_type=jnp.float32
    )
    return jnp.where(low, mixed[:GRID_W], mixed[GRID_W:]).astype(jnp.bfloat16)


def row_window(row, rows_dev, rows_all):
    reach = NA_ROWS // 2
    row_base = lax.axis_index("sp") * rows_dev
    first = jnp.clip(row_base + row - reach, 0, rows_all - NA_ROWS)
    return first - row_base + reach, first - row_base - row + NA_ROWS - 1


MESH = pl.DeviceIdType.MESH
LAG = 3


def tp_copy(src, dst, sems, index, peer):
    return pltpu.make_async_remote_copy(
        src_ref=src,
        dst_ref=dst,
        send_sem=sems.at[0, index],
        recv_sem=sems.at[1, index],
        device_id=(lax.axis_index("sp"), peer),
        device_id_type=MESH,
    )


class SquareGather:
    def __init__(self, slots, sems, chunks):
        self.slots, self.sems, self.chunks = slots, sems, chunks
        self.rows = slots.shape[1] // chunks
        self.me = lax.axis_index("tp")
        self.across = self.me + 1 - 2 * (self.me % 2)
        self.over = (self.me + 2) % 4
        self.corner = (self.across + 2) % 4

    def part(self, slot, chunk):
        start = chunk * self.rows
        if not isinstance(chunk, int):
            start = pl.multiple_of(start, self.rows)
        return self.slots.at[slot, pl.ds(start, self.rows), :]

    def copy(self, kind, slot, chunk, peer):
        part = self.part(slot, chunk)
        return tp_copy(part, part, self.sems.at[kind], chunk, peer)

    def send(self, chunk):
        self.copy(0, self.me, chunk, self.across).start()
        self.copy(1, self.me, chunk, self.over).start()

    def relay(self, chunk):
        self.copy(0, self.across, chunk, self.across).wait_recv()
        self.copy(1, self.over, chunk, self.over).wait_recv()

        @pl.when(chunk % 2 == 0)
        def _():
            self.copy(2, self.across, chunk, self.over).start()

        @pl.when(chunk % 2 == 1)
        def _():
            self.copy(2, self.over, chunk, self.across).start()

    def finish(self, chunk):
        self.copy(2, self.corner, chunk, self.over).wait_recv()

    def drain(self):
        def one(chunk, carry):
            self.copy(0, self.me, chunk, self.across).wait_send()
            self.copy(1, self.me, chunk, self.over).wait_send()
            self.copy(2, self.across, chunk, self.over).wait_send()
            return carry

        lax.fori_loop(0, self.chunks, one, 0)


def stack_kernel(
    rows_dev, rows_all,
    x_ref, gain_ref, lanes_ref, wq_ref, wk_ref, wv_ref, wo_ref, out_ref,
    gains, weights, stream, mixed, keyval, queries, normed, tables,
    partial, weight_sems, gain_sems, stream_sems, mixed_sems, halo_sems,
):
    sp, sp_size = lax.axis_index("sp"), lax.axis_size("sp")
    layers = wq_ref.shape[0]
    tokens, feats = x_ref.shape
    width = feats
    reach = NA_ROWS // 2 * GRID_W
    streams = SquareGather(stream, stream_sems, rows_dev)
    mixes = SquareGather(mixed, mixed_sems, rows_dev)
    me, across, over = streams.me, streams.across, streams.over
    corner = streams.corner
    sources = (wk_ref, wv_ref, wq_ref, wo_ref)

    def weight_copy(kind, layer):
        return pltpu.make_async_copy(
            sources[kind].at[layer], weights.at[kind, layer], weight_sems.at[kind, layer]
        )

    for layer in range(layers):
        for kind in range(4):
            weight_copy(kind, layer).start()

    barrier = pltpu.get_barrier_semaphore()
    for peer in (across, over, corner):
        pl.semaphore_signal(barrier, inc=1, device_id=(sp, peer), device_id_type=MESH)

    @pl.when(sp > 0)
    def _():
        pl.semaphore_signal(barrier, inc=1, device_id=(sp - 1, me), device_id_type=MESH)

    @pl.when(sp < sp_size - 1)
    def _():
        pl.semaphore_signal(barrier, inc=1, device_id=(sp + 1, me), device_id_type=MESH)

    stream[me] = x_ref[...]
    gains[me, 0:layers, :] = gain_ref[...].astype(jnp.float32)
    sides = jnp.minimum(sp, 1) + jnp.minimum(sp_size - 1 - sp, 1)
    pl.semaphore_wait(barrier, 3 + sides)

    def gain_copy(index, slot, peer):
        return tp_copy(gains.at[slot], gains.at[slot], gain_sems, index, peer)

    for index, peer in enumerate((across, over, corner)):
        gain_copy(index, me, peer).start()

    pairs = rows_dev // 2
    tall = 2 * GRID_W
    parts = NA_ROWS // 4
    down_parts = range(parts)
    up_parts = range(pairs - parts, pairs)
    order = sorted(range(pairs), key=lambda j: -((j in down_parts) + (j in up_parts)))

    def halo_copy(parity, up, part, kind):
        cols = slice(kind * width, (kind + 1) * width)
        local = reach + (pairs - parts + part if up else part) * tall
        there = part * tall + (0 if up else tokens + reach)
        return pltpu.make_async_remote_copy(
            src_ref=keyval.at[parity, pl.ds(local, tall), cols],
            dst_ref=keyval.at[parity, pl.ds(there, tall), cols],
            send_sem=halo_sems.at[0, parity, int(up), part, kind],
            recv_sem=halo_sems.at[1, parity, int(up), part, kind],
            device_id=(sp + 1 if up else sp - 1, me),
            device_id_type=MESH,
        )

    def send_halo(parity, pair, kind):
        if pair in down_parts:

            @pl.when(sp > 0)
            def _():
                halo_copy(parity, False, pair, kind).start()

        if pair in up_parts:

            @pl.when(sp < sp_size - 1)
            def _():
                halo_copy(parity, True, pair - (pairs - parts), kind).start()

    def one_layer(layer, carry):
        parity = layer % 2
        for pair in order[:2]:
            streams.send(2 * pair)
            streams.send(2 * pair + 1)
        for pair in range(width // 128):
            build_table(
                lambda off: lanes_ref[layer, pair, off : off + 1, :], tables.at[pair]
            )

        def relay_pair(pair):
            streams.relay(2 * pair)
            streams.relay(2 * pair + 1)

        def norm_pair(pair):
            here = slice(pair * tall, (pair + 1) * tall)
            total = jnp.zeros((tall, 1), jnp.float32)
            for slot in range(4):
                part = stream[slot, here, :].astype(jnp.float32)
                total += jnp.sum(part * part, axis=1, keepdims=True)
            inverse = lax.rsqrt(total * (1.0 / (4 * feats)) + epsilon)
            for slot in range(4):
                part = stream[slot, here, :].astype(jnp.float32)
                gain = gains[slot, pl.ds(layer, 1), :]
                normed[here, slot * feats : (slot + 1) * feats] = (
                    part * inverse * gain
                ).astype(jnp.bfloat16)

        def project_pair(pair):
            here = slice(pair * tall, (pair + 1) * tall)
            there = slice(reach + pair * tall, reach + (pair + 1) * tall)
            for kind in range(2):
                keyval[parity, there, kind * width : (kind + 1) * width] = contract(
                    normed[here, :], weights[kind, layer]
                ).astype(jnp.bfloat16)
                send_halo(parity, pair, kind)
            queries[here, :] = contract(normed[here, :], weights[2, layer]).astype(
                jnp.bfloat16
            ) * jnp.bfloat16(HEAD_DIM ** (-0.5))

        @pl.when(layer == 0)
        def _():
            for index, peer in enumerate((across, over, corner)):
                gain_copy(index, peer, peer).wait_recv()
                gain_copy(index, me, peer).wait_send()

        for kind in range(3):
            weight_copy(kind, layer).wait()
        relay_pair(order[0])
        for pair in order[2:]:
            streams.send(2 * pair)
            streams.send(2 * pair + 1)
        for place, pair in enumerate(order):
            if place + 1 < pairs:
                relay_pair(order[place + 1])
            streams.finish(2 * pair)
            streams.finish(2 * pair + 1)
            norm_pair(pair)
            project_pair(pair)
        streams.drain()

        def wait_halo(up):
            for part in range(parts):
                for kind in range(2):
                    halo_copy(parity, up, part, kind).wait_recv()

        @pl.when(sp < sp_size - 1)
        def _():
            wait_halo(False)

        @pl.when((sp > 0) & (sp == sp_size - 1))
        def _():
            wait_halo(True)

        def one_row(step, carry):
            row = rows_dev - 1 - step

            @pl.when((step == rows_dev - NA_ROWS // 2) & (sp > 0) & (sp < sp_size - 1))
            def _():
                wait_halo(True)

            start, off = row_window(row, rows_dev, rows_all)
            keys = pl.ds(pl.multiple_of(start * GRID_W, GRID_W), NA_ROWS * GRID_W)
            here = pl.ds(pl.multiple_of(row * GRID_W, GRID_W), GRID_W)
            offs = pl.ds(pl.multiple_of(off * GRID_W, GRID_W), NA_ROWS * GRID_W)
            for pair in range(width // 128):
                cols = slice(pair * 128, (pair + 1) * 128)
                vcols = slice(width + pair * 128, width + (pair + 1) * 128)
                mixed[me, here, cols] = attend_row(
                    queries[here, cols],
                    keyval[parity, keys, cols],
                    keyval[parity, keys, vcols],
                    tables[pair, offs, :],
                )
            mixes.send(row)

            @pl.when(step >= LAG)
            def _():
                mixes.relay(row + LAG)

            return carry

        lax.fori_loop(0, rows_dev, one_row, 0)

        def relay_rest(step, carry):
            mixes.relay(rows_dev - 1 - step)
            return carry

        lax.fori_loop(rows_dev - LAG, rows_dev, relay_rest, 0)
        weight_copy(3, layer).wait()

        def out_part(slot):
            cols = pl.ds(pl.multiple_of(slot * width, width), width)
            return contract(mixed[slot], weights[3, layer, :, cols])

        total = stream[me].astype(jnp.float32) + out_part(me)
        partial[...] = total + out_part(across) + out_part(over)

        for part in range(parts):
            for kind in range(2):

                @pl.when(sp > 0)
                def _():
                    halo_copy(parity, False, part, kind).wait_send()

                @pl.when(sp < sp_size - 1)
                def _():
                    halo_copy(parity, True, part, kind).wait_send()

        def finish_chunk(chunk, carry):
            mixes.finish(chunk)
            return carry

        lax.fori_loop(0, rows_dev, finish_chunk, 0)
        mixes.drain()
        total = partial[...] + out_part(corner)
        stream[me] = total.astype(jnp.bfloat16)
        return carry

    lax.fori_loop(0, layers, one_layer, 0)
    out_ref[...] = stream[me]


def square_device(residual, norm_gain, w_query, w_key, w_value, w_out, offset_bias):
    tokens, feats = residual.shape
    layers = w_query.shape[0]
    rows_dev = tokens // GRID_W
    rows_all = rows_dev * lax.axis_size("sp")
    lanes = bias_lanes(offset_bias)
    vmem = pl.BlockSpec(memory_space=pltpu.VMEM)
    hbm = pl.BlockSpec(memory_space=pl.ANY)
    bf16, dma = jnp.bfloat16, pltpu.SemaphoreType.DMA
    padded = tokens + NA_ROWS * GRID_W
    return pl.pallas_call(
        lambda *refs: stack_kernel(rows_dev, rows_all, *refs),
        out_shape=jax.ShapeDtypeStruct(residual.shape, bf16),
        in_specs=[vmem] * 3 + [hbm] * 4,
        out_specs=vmem,
        scratch_shapes=[
            pltpu.VMEM((4, -(-layers // 8) * 8, feats), jnp.float32),
            pltpu.VMEM((4,) + w_query.shape, bf16),
            pltpu.VMEM((4, tokens, feats), bf16),
            pltpu.VMEM((4, tokens, feats), bf16),
            pltpu.VMEM((2, padded, 2 * feats), bf16),
            pltpu.VMEM((tokens, feats), bf16),
            pltpu.VMEM((tokens, 4 * feats), bf16),
            pltpu.VMEM((feats // 128, (2 * NA_ROWS - 1) * GRID_W, 128), jnp.float32),
            pltpu.VMEM((tokens, feats), jnp.float32),
            dma((4, layers)),
            dma((2, 3)),
            dma((3, 2, rows_dev)),
            dma((3, 2, rows_dev)),
            dma((2, 2, 2, NA_ROWS // 4, 2)),
        ],
        compiler_params=pltpu.CompilerParams(
            collective_id=0, has_side_effects=True, vmem_limit_bytes=56 * 1024 * 1024
        ),
        name="stack",
    )(residual, norm_gain, lanes, w_query, w_key, w_value, w_out)


def per_device(residual, norm_gain, w_query, w_key, w_value, w_out, offset_bias):
    paired = offset_bias.shape[1] % 2 == 0 and 2 * HEAD_DIM == 128 and 2 * GRID_W == 128
    square = lax.axis_size("tp") == 4 and offset_bias.shape[1] * HEAD_DIM == residual.shape[1]
    rows_dev = residual.shape[0] // GRID_W
    even = rows_dev % 2 == 0 and rows_dev >= NA_ROWS // 2
    body = generic_device
    if paired and square and even:
        body = square_device
    return body(residual, norm_gain, w_query, w_key, w_value, w_out, offset_bias)


def solution(mesh):
    in_specs = (
        P("sp", "tp"),
        P(None, "tp"),
        P(None, "tp", None),
        P(None, "tp", None),
        P(None, "tp", None),
        P(None, "tp", None),
        P(None, "tp", None, None),
    )
    out_specs = P("sp", "tp")
    return jax.shard_map(
        per_device, mesh=mesh, in_specs=in_specs, out_specs=out_specs, check_vma=False
    )
```

```python
import jax
import jax.numpy as jnp
from jax import lax
from jax.experimental import pallas as pl
from jax.experimental.pallas import tpu as pltpu
from jax.sharding import PartitionSpec as P

HEAD_DIM = 64
GRID_W = 64
NA_ROWS = 8
NA_COLS = 16
LAYERS = 3


epsilon = 1e-06


def padded_2(array, sides, width):
    for axis, dim in sides:
        size, length = (lax.axis_size(axis), array.shape[dim])
        up = [(i, (i + 1) % size) for i in range(size - 1)]
        down = [(j, i) for i, j in up]
        last = lax.slice_in_dim(array, length - width, length, axis=dim)
        first = lax.slice_in_dim(array, 0, width, axis=dim)
        before = lax.ppermute(last, axis, up)
        after = lax.ppermute(first, axis, down)
        array = jnp.concatenate([before, array, after], axis=dim)
    return array


def shortened(array):
    return jax.tree.map(lambda a: a.astype(jnp.bfloat16) if a.dtype == jnp.float32 else a, array)


def contract(left, right):
    return lax.dot_general(
        left, right, (((1,), (1,)), ((), ())), preferred_element_type=jnp.float32
    )


def generic_device(residual, norm_gain, w_query, w_key, w_value, w_out, offset_bias):
    token_count = residual.shape[0]
    local_feats = residual.shape[1]
    local_heads = offset_bias.shape[1]
    head_cols = local_heads * HEAD_DIM
    rows_dev = token_count // GRID_W
    rows_all = rows_dev * lax.axis_size("sp")
    row_base = lax.axis_index("sp") * rows_dev
    reach = NA_ROWS // 2
    slab_width = min(2 * NA_COLS, GRID_W)
    tile_starts = list(range(0, GRID_W, NA_COLS))
    slab_starts = [min(max(start - NA_COLS // 2, 0), GRID_W - slab_width) for start in tile_starts]
    tile_info = []
    for start, slab in zip(tile_starts, slab_starts):
        query_cols = start + jnp.arange(NA_COLS, dtype=jnp.int32)
        key_cols = slab + jnp.arange(slab_width, dtype=jnp.int32)
        first_col = jnp.clip(query_cols - NA_COLS // 2, 0, GRID_W - NA_COLS)
        inside = (key_cols[None, :] >= first_col[:, None]) & (
            key_cols[None, :] < first_col[:, None] + NA_COLS
        )
        offsets = key_cols[None, :] - query_cols[:, None] + (NA_COLS - 1)
        onehot = (offsets[:, :, None] == jnp.arange(2 * NA_COLS - 1, dtype=jnp.int32)).astype(
            jnp.float32
        )
        tile_info.append((start, slab, inside, onehot))
    stream = residual
    for layer_index in range(LAYERS):
        res_float = stream.astype(jnp.float32)
        gathered, gain_all = (
            lax.all_gather(stream, "tp", axis=1, tiled=True),
            lax.all_gather(norm_gain[layer_index][None, :], "tp", axis=1, tiled=True),
        )
        full_float = gathered.astype(jnp.float32)
        inverse = lax.rsqrt(jnp.mean(full_float * full_float, axis=1, keepdims=True) + epsilon)
        normed_all = (full_float * inverse * gain_all.astype(jnp.float32)).astype(jnp.bfloat16)
        queries = contract(normed_all, w_query[layer_index])
        keys = contract(normed_all, w_key[layer_index])
        values = contract(normed_all, w_value[layer_index])
        queries = queries.astype(jnp.bfloat16)
        key_value = jnp.concatenate(
            [keys.astype(jnp.bfloat16), values.astype(jnp.bfloat16)], axis=1
        )
        padded = padded_2(key_value, (("sp", 0),), reach * GRID_W)
        key_grid = padded.reshape(rows_dev + 2 * reach, GRID_W, 2, local_heads, HEAD_DIM)
        query_grid = queries.reshape(rows_dev, GRID_W, local_heads, HEAD_DIM)
        lookup = offset_bias[layer_index]

        def one_row(row_index, query_row):
            row_global = row_base + row_index
            first_row = jnp.clip(row_global - reach, 0, rows_all - NA_ROWS)
            local_first = first_row - row_base + reach
            window = lax.dynamic_slice_in_dim(key_grid, local_first, NA_ROWS, 0)
            row_offset = (
                first_row + jnp.arange(NA_ROWS, dtype=jnp.int32) - row_global + (NA_ROWS - 1)
            )
            row_onehot = (
                row_offset[:, None] == jnp.arange(2 * NA_ROWS - 1, dtype=jnp.int32)
            ).astype(jnp.float32)
            row_bias = jnp.einsum(
                "hab,ra->hrb", lookup, row_onehot, precision=lax.Precision.HIGHEST
            )
            pieces = []
            for start, slab, inside, onehot in tile_info:
                query_tile = query_row[start : start + NA_COLS]
                slab_keys = window[:, slab : slab + slab_width, 0]
                slab_values = window[:, slab : slab + slab_width, 1]
                bias_terms = jnp.einsum(
                    "hrb,wsb->hwrs", row_bias, onehot, precision=lax.Precision.HIGHEST
                )
                scores = jnp.einsum(
                    "whd,rshd->hwrs", query_tile, slab_keys, preferred_element_type=jnp.float32
                )
                scores = scores * HEAD_DIM ** (-0.5) + bias_terms
                scores = jnp.where(inside[None, :, None, :], scores, -jnp.inf)
                weights = jax.nn.softmax(
                    scores.reshape(local_heads, NA_COLS, NA_ROWS * slab_width), axis=-1
                ).astype(jnp.bfloat16)
                weights = weights.reshape(local_heads, NA_COLS, NA_ROWS, slab_width)
                attended = jnp.einsum(
                    "hwrs,rshd->whd", weights, slab_values, preferred_element_type=jnp.float32
                )
                pieces.append(attended.astype(jnp.bfloat16).reshape(NA_COLS, head_cols))
            return jnp.concatenate(pieces, axis=0)

        attended = jax.vmap(one_row)(jnp.arange(rows_dev, dtype=jnp.int32), query_grid).reshape(
            token_count, head_cols
        )
        portion = jax.tree.map(
            lambda part: lax.all_gather(part, "tp", axis=1, tiled=True), shortened(attended)
        )
        out_rows = lax.slice_in_dim(w_out[layer_index], 0, portion.shape[1], axis=1)
        mixed = jnp.zeros((token_count, local_feats), jnp.float32) + contract(portion, out_rows)
        stream = (res_float + mixed).astype(jnp.bfloat16)
    return stream


def bias_lanes(offset_bias):
    layers, heads, row_offs, col_offs = offset_bias.shape
    flipped = jnp.flip(offset_bias, axis=3)
    padded = jnp.pad(flipped, ((0, 0), (0, 0), (0, 1), (0, GRID_W - col_offs)))
    paired = padded.reshape(layers, heads // 2, 2, row_offs + 1, GRID_W)
    return paired.transpose(0, 1, 3, 2, 4).reshape(layers, heads // 2, row_offs + 1, 2 * GRID_W)


def window_mask():
    shape = (GRID_W, 2 * GRID_W)
    key_col = lax.broadcasted_iota(jnp.int32, shape, 0)
    query_col = lax.broadcasted_iota(jnp.int32, shape, 1) % GRID_W
    first = jnp.clip(query_col - NA_COLS // 2, 0, GRID_W - NA_COLS)
    return (key_col >= first) & (key_col < first + NA_COLS)


def build_table(lanes_of, table):
    inside = window_mask()
    for off in range(2 * NA_ROWS - 1):
        row = jnp.broadcast_to(lanes_of(off), (GRID_W, 2 * GRID_W))
        rolled = pltpu.roll(row, 2 * GRID_W - (NA_COLS - 1), axis=1, stride=1, stride_axis=0)
        table[off * GRID_W : (off + 1) * GRID_W, :] = jnp.where(inside, rolled, -1e30)


def attend_row(query, window_keys, window_values, bias):
    low = lax.broadcasted_iota(jnp.int32, query.shape, 1) < HEAD_DIM
    zero = jnp.zeros_like(query)
    block = jnp.concatenate([jnp.where(low, query, zero), jnp.where(low, zero, query)], axis=0)
    scores = contract(window_keys, block) + bias
    top = jnp.max(scores, axis=0, keepdims=True)
    weights = jnp.exp(scores - top)
    inverse = 1.0 / jnp.sum(weights, axis=0, keepdims=True)
    weights = (weights * inverse).astype(jnp.bfloat16)
    mixed = lax.dot_general(
        weights, window_values, (((0,), (0,)), ((), ())), preferred_element_type=jnp.float32
    )
    return jnp.where(low, mixed[:GRID_W], mixed[GRID_W:]).astype(jnp.bfloat16)


def row_window(row, rows_dev, rows_all):
    reach = NA_ROWS // 2
    row_base = lax.axis_index("sp") * rows_dev
    first = jnp.clip(row_base + row - reach, 0, rows_all - NA_ROWS)
    return first - row_base + reach, first - row_base - row + NA_ROWS - 1


MESH = pl.DeviceIdType.MESH
LAG = 3


def tp_copy(src, dst, sems, index, peer):
    return pltpu.make_async_remote_copy(
        src_ref=src,
        dst_ref=dst,
        send_sem=sems.at[0, index],
        recv_sem=sems.at[1, index],
        device_id=(lax.axis_index("sp"), peer),
        device_id_type=MESH,
    )


class SquareGather:
    def __init__(self, slots, sems, chunks):
        self.slots, self.sems, self.chunks = slots, sems, chunks
        self.rows = slots.shape[1] // chunks
        self.me = lax.axis_index("tp")
        self.across = self.me + 1 - 2 * (self.me % 2)
        self.over = (self.me + 2) % 4
        self.corner = (self.across + 2) % 4

    def part(self, slot, chunk):
        start = chunk * self.rows
        if not isinstance(chunk, int):
            start = pl.multiple_of(start, self.rows)
        return self.slots.at[slot, pl.ds(start, self.rows), :]

    def copy(self, kind, slot, chunk, peer):
        part = self.part(slot, chunk)
        return tp_copy(part, part, self.sems.at[kind], chunk, peer)

    def send(self, chunk):
        self.copy(0, self.me, chunk, self.across).start()
        self.copy(1, self.me, chunk, self.over).start()

    def relay(self, chunk):
        self.copy(0, self.across, chunk, self.across).wait_recv()
        self.copy(1, self.over, chunk, self.over).wait_recv()

        @pl.when(chunk % 2 == 0)
        def _():
            self.copy(2, self.across, chunk, self.over).start()

        @pl.when(chunk % 2 == 1)
        def _():
            self.copy(2, self.over, chunk, self.across).start()

    def finish(self, chunk):
        self.copy(2, self.corner, chunk, self.over).wait_recv()

    def drain(self):
        def one(chunk, carry):
            self.copy(0, self.me, chunk, self.across).wait_send()
            self.copy(1, self.me, chunk, self.over).wait_send()
            self.copy(2, self.across, chunk, self.over).wait_send()
            return carry

        lax.fori_loop(0, self.chunks, one, 0)


def stack_kernel(
    rows_dev, rows_all,
    x_ref, gain_ref, lanes_ref, wq_ref, wk_ref, wv_ref, wo_ref, out_ref,
    gains, weights, stream, mixed, keyval, queries, normed, tables,
    partial, weight_sems, gain_sems, stream_sems, mixed_sems, halo_sems,
):
    sp, sp_size = lax.axis_index("sp"), lax.axis_size("sp")
    layers = wq_ref.shape[0]
    tokens, feats = x_ref.shape
    width = feats
    reach = NA_ROWS // 2 * GRID_W
    streams = SquareGather(stream, stream_sems, rows_dev)
    mixes = SquareGather(mixed, mixed_sems, rows_dev)
    me, across, over = streams.me, streams.across, streams.over
    corner = streams.corner
    sources = (wk_ref, wv_ref, wq_ref, wo_ref)

    def weight_copy(kind, layer):
        return pltpu.make_async_copy(
            sources[kind].at[layer], weights.at[kind, layer], weight_sems.at[kind, layer]
        )

    for layer in range(layers):
        for kind in range(4):
            weight_copy(kind, layer).start()

    barrier = pltpu.get_barrier_semaphore()
    for peer in (across, over, corner):
        pl.semaphore_signal(barrier, inc=1, device_id=(sp, peer), device_id_type=MESH)

    @pl.when(sp > 0)
    def _():
        pl.semaphore_signal(barrier, inc=1, device_id=(sp - 1, me), device_id_type=MESH)

    @pl.when(sp < sp_size - 1)
    def _():
        pl.semaphore_signal(barrier, inc=1, device_id=(sp + 1, me), device_id_type=MESH)

    stream[me] = x_ref[...]
    gains[me, 0:layers, :] = gain_ref[...].astype(jnp.float32)
    sides = jnp.minimum(sp, 1) + jnp.minimum(sp_size - 1 - sp, 1)
    pl.semaphore_wait(barrier, 3 + sides)

    def gain_copy(index, slot, peer):
        return tp_copy(gains.at[slot], gains.at[slot], gain_sems, index, peer)

    for index, peer in enumerate((across, over, corner)):
        gain_copy(index, me, peer).start()

    pairs = rows_dev // 2
    tall = 2 * GRID_W
    parts = NA_ROWS // 4
    down_parts = range(parts)
    up_parts = range(pairs - parts, pairs)
    order = sorted(range(pairs), key=lambda j: -((j in down_parts) + (j in up_parts)))

    def halo_copy(parity, up, part, kind):
        cols = slice(kind * width, (kind + 1) * width)
        local = reach + (pairs - parts + part if up else part) * tall
        there = part * tall + (0 if up else tokens + reach)
        return pltpu.make_async_remote_copy(
            src_ref=keyval.at[parity, pl.ds(local, tall), cols],
            dst_ref=keyval.at[parity, pl.ds(there, tall), cols],
            send_sem=halo_sems.at[0, parity, int(up), part, kind],
            recv_sem=halo_sems.at[1, parity, int(up), part, kind],
            device_id=(sp + 1 if up else sp - 1, me),
            device_id_type=MESH,
        )

    def send_halo(parity, pair, kind):
        if pair in down_parts:

            @pl.when(sp > 0)
            def _():
                halo_copy(parity, False, pair, kind).start()

        if pair in up_parts:

            @pl.when(sp < sp_size - 1)
            def _():
                halo_copy(parity, True, pair - (pairs - parts), kind).start()

    def send_pair(pair):
        streams.send(2 * pair)
        streams.send(2 * pair + 1)

    for pair in order[:2]:
        send_pair(pair)

    def one_layer(layer, carry):
        parity = layer % 2
        for pair in range(width // 128):
            build_table(
                lambda off: lanes_ref[layer, pair, off : off + 1, :], tables.at[pair]
            )

        def relay_pair(pair):
            streams.relay(2 * pair)
            streams.relay(2 * pair + 1)

        def norm_pair(pair):
            here = slice(pair * tall, (pair + 1) * tall)
            total = jnp.zeros((tall, 1), jnp.float32)
            for slot in range(4):
                part = stream[slot, here, :].astype(jnp.float32)
                total += jnp.sum(part * part, axis=1, keepdims=True)
            inverse = lax.rsqrt(total * (1.0 / (4 * feats)) + epsilon)
            for slot in range(4):
                part = stream[slot, here, :].astype(jnp.float32)
                gain = gains[slot, pl.ds(layer, 1), :]
                normed[here, slot * feats : (slot + 1) * feats] = (
                    part * inverse * gain
                ).astype(jnp.bfloat16)

        def project_pair(pair):
            here = slice(pair * tall, (pair + 1) * tall)
            there = slice(reach + pair * tall, reach + (pair + 1) * tall)
            for kind in range(2):
                keyval[parity, there, kind * width : (kind + 1) * width] = contract(
                    normed[here, :], weights[kind, layer]
                ).astype(jnp.bfloat16)
                send_halo(parity, pair, kind)
            queries[here, :] = contract(normed[here, :], weights[2, layer]).astype(
                jnp.bfloat16
            ) * jnp.bfloat16(HEAD_DIM ** (-0.5))

        @pl.when(layer == 0)
        def _():
            for index, peer in enumerate((across, over, corner)):
                gain_copy(index, peer, peer).wait_recv()
                gain_copy(index, me, peer).wait_send()

        for kind in range(3):
            weight_copy(kind, layer).wait()
        relay_pair(order[0])
        for pair in order[2:]:
            streams.send(2 * pair)
            streams.send(2 * pair + 1)
        for place, pair in enumerate(order):
            if place + 1 < pairs:
                relay_pair(order[place + 1])
            streams.finish(2 * pair)
            streams.finish(2 * pair + 1)
            norm_pair(pair)
            project_pair(pair)
        streams.drain()

        def wait_halo(up):
            for part in range(parts):
                for kind in range(2):
                    halo_copy(parity, up, part, kind).wait_recv()

        @pl.when(sp < sp_size - 1)
        def _():
            wait_halo(False)

        @pl.when((sp > 0) & (sp == sp_size - 1))
        def _():
            wait_halo(True)

        def one_row(step, carry):
            row = rows_dev - 1 - step

            @pl.when((step == rows_dev - NA_ROWS // 2) & (sp > 0) & (sp < sp_size - 1))
            def _():
                wait_halo(True)

            start, off = row_window(row, rows_dev, rows_all)
            keys = pl.ds(pl.multiple_of(start * GRID_W, GRID_W), NA_ROWS * GRID_W)
            here = pl.ds(pl.multiple_of(row * GRID_W, GRID_W), GRID_W)
            offs = pl.ds(pl.multiple_of(off * GRID_W, GRID_W), NA_ROWS * GRID_W)
            for pair in range(width // 128):
                cols = slice(pair * 128, (pair + 1) * 128)
                vcols = slice(width + pair * 128, width + (pair + 1) * 128)
                mixed[me, here, cols] = attend_row(
                    queries[here, cols],
                    keyval[parity, keys, cols],
                    keyval[parity, keys, vcols],
                    tables[pair, offs, :],
                )
            mixes.send(row)

            @pl.when(step >= LAG)
            def _():
                mixes.relay(row + LAG)

            return carry

        lax.fori_loop(0, rows_dev, one_row, 0)

        def relay_rest(step, carry):
            mixes.relay(rows_dev - 1 - step)
            return carry

        lax.fori_loop(rows_dev - LAG, rows_dev, relay_rest, 0)
        weight_copy(3, layer).wait()

        def out_part(slot):
            cols = pl.ds(pl.multiple_of(slot * width, width), width)
            return contract(mixed[slot], weights[3, layer, :, cols])

        total = stream[me].astype(jnp.float32) + out_part(me)
        partial[...] = total + out_part(across) + out_part(over)

        for part in range(parts):
            for kind in range(2):

                @pl.when(sp > 0)
                def _():
                    halo_copy(parity, False, part, kind).wait_send()

                @pl.when(sp < sp_size - 1)
                def _():
                    halo_copy(parity, True, part, kind).wait_send()

        def finish_chunk(chunk, carry):
            mixes.finish(chunk)
            return carry

        lax.fori_loop(0, rows_dev, finish_chunk, 0)
        mixes.drain()
        corner_cols = pl.ds(pl.multiple_of(corner * width, width), width)
        for place, pair in enumerate(order):
            here = slice(pair * tall, (pair + 1) * tall)
            last = contract(mixed[corner, here, :], weights[3, layer, :, corner_cols])
            stream[me, here, :] = (partial[here, :] + last).astype(jnp.bfloat16)
            if place < 2:

                @pl.when(layer < layers - 1)
                def _():
                    send_pair(pair)

        return carry

    lax.fori_loop(0, layers, one_layer, 0)
    out_ref[...] = stream[me]


def square_device(residual, norm_gain, w_query, w_key, w_value, w_out, offset_bias):
    tokens, feats = residual.shape
    layers = w_query.shape[0]
    rows_dev = tokens // GRID_W
    rows_all = rows_dev * lax.axis_size("sp")
    lanes = bias_lanes(offset_bias)
    vmem = pl.BlockSpec(memory_space=pltpu.VMEM)
    hbm = pl.BlockSpec(memory_space=pl.ANY)
    bf16, dma = jnp.bfloat16, pltpu.SemaphoreType.DMA
    padded = tokens + NA_ROWS * GRID_W
    return pl.pallas_call(
        lambda *refs: stack_kernel(rows_dev, rows_all, *refs),
        out_shape=jax.ShapeDtypeStruct(residual.shape, bf16),
        in_specs=[vmem] * 3 + [hbm] * 4,
        out_specs=vmem,
        scratch_shapes=[
            pltpu.VMEM((4, -(-layers // 8) * 8, feats), jnp.float32),
            pltpu.VMEM((4,) + w_query.shape, bf16),
            pltpu.VMEM((4, tokens, feats), bf16),
            pltpu.VMEM((4, tokens, feats), bf16),
            pltpu.VMEM((2, padded, 2 * feats), bf16),
            pltpu.VMEM((tokens, feats), bf16),
            pltpu.VMEM((tokens, 4 * feats), bf16),
            pltpu.VMEM((feats // 128, (2 * NA_ROWS - 1) * GRID_W, 128), jnp.float32),
            pltpu.VMEM((tokens, feats), jnp.float32),
            dma((4, layers)),
            dma((2, 3)),
            dma((3, 2, rows_dev)),
            dma((3, 2, rows_dev)),
            dma((2, 2, 2, NA_ROWS // 4, 2)),
        ],
        compiler_params=pltpu.CompilerParams(
            collective_id=0, has_side_effects=True, vmem_limit_bytes=56 * 1024 * 1024
        ),
        name="stack",
    )(residual, norm_gain, lanes, w_query, w_key, w_value, w_out)


def per_device(residual, norm_gain, w_query, w_key, w_value, w_out, offset_bias):
    paired = offset_bias.shape[1] % 2 == 0 and 2 * HEAD_DIM == 128 and 2 * GRID_W == 128
    square = lax.axis_size("tp") == 4 and offset_bias.shape[1] * HEAD_DIM == residual.shape[1]
    rows_dev = residual.shape[0] // GRID_W
    even = rows_dev % 2 == 0 and rows_dev >= NA_ROWS // 2
    body = generic_device
    if paired and square and even:
        body = square_device
    return body(residual, norm_gain, w_query, w_key, w_value, w_out, offset_bias)


def solution(mesh):
    in_specs = (
        P("sp", "tp"),
        P(None, "tp"),
        P(None, "tp", None),
        P(None, "tp", None),
        P(None, "tp", None),
        P(None, "tp", None),
        P(None, "tp", None, None),
    )
    out_specs = P("sp", "tp")
    return jax.shard_map(
        per_device, mesh=mesh, in_specs=in_specs, out_specs=out_specs, check_vma=False
    )
```
